32 devices in a mesh: ep: 4 (over y, x), tp: 8 (over z, core).
Axes of the slice: x: 2, y: 2, z: 4, core: 2. Of those that a mesh axis runs over, the one named last changes fastest.
Arguments:
- pool_in: bfloat16 [16384, 1024], P(('ep', 'tp')), may hold values from -6 to 6
- pool_weight: bfloat16 [4, 256, 256], replicated, may hold values from -0.375 to 0.375
- pool_gain: float32 [1024], replicated, may hold values from 0.1 to 1.9
- out_weight: bfloat16 [1024, 2048], P('tp'), may hold values from -0.1875 to 0.1875
- mix_gain: float32 [2048], replicated, may hold values from 0.1 to 1.9
- expert_in: bfloat16 [1024, 2048], P('ep'), may hold values from -6 to 6
- routes: int32 [1024, 4], P('ep'), may hold values from 0 to 7, all different within a row; in each aligned block of 32 rows (0 to 31, 32 to 63, ...) at most 32 rows name the same one
- route_weight: float32 [1024, 4], P('ep'), may hold values from 0.1 to 1
- pre_gain: float32 [2048], replicated, may hold values from 0.1 to 1.9
- gate_weight: bfloat16 [8, 2048, 4096], P('ep', None, 'tp'), may hold values from -0.39648438 to 0.39648438
- up_weight: bfloat16 [8, 2048, 4096], P('ep', None, 'tp'), may hold values from -0.39648438 to 0.39648438
- down_weight: bfloat16 [8, 4096, 2048], P('ep', 'tp'), may hold values from -0.09375 to 0.09375
- post_gain: float32 [2048], replicated, may hold values from 0.1 to 1.9
Outputs:
- mix_out: bfloat16 [16384, 2048], P(('ep', 'tp'))
- expert_out: bfloat16 [1024, 2048], P(('ep', 'tp'))
The draws below stay inside these ranges and needn't reach their ends.
Inputs may be any that keep to these rules, and one draw needn't show every extreme that they name: `routes`: each row names 4 different experts. In each aligned block of 32 rows no expert is named by more than 32 rows, a bound that some block reaches.
All inputs are finite; a program needn't handle non-finite values.
Results may differ from the reference program's by a relative error of at most 0.019.
Values may be sent and summed in bfloat16 or wider, within the bound.
No kernel may reach another device: no remote copies, remote signals or barrier semaphores. Data moves between devices by JAX's collectives and lax.ppermute only.
A program may use at most 128 MiB of HBM per device.

```python
import math
import jax
import jax.numpy as jnp
import numpy as np
from jax import lax

D = 2048
DP = 1024
GROUP = 256
FF = 4096
EXPERTS = 8
TOPK = 4
MOE_TOK = 1024
MIX_TOK = 16384
SUB = 32
CAP = 32
N_TP = 8


def shard_levels(rng, dims, cuts, least, high):
    level, own = 1.0, jax.random.fold_in(rng, 6)
    for dim, shards_of in cuts:
        heights = jnp.exp(jax.random.uniform(jax.random.fold_in(own, dim), (shards_of,), jnp.float32, least / len(cuts), high / len(cuts)))
        level = level * jnp.repeat(heights, dims[dim] // shards_of).reshape([-1 if axis == dim else 1 for axis in range(len(dims))])
    return level


def deal_out(rng, own, number, rows, count, top, most, lean):
    order = jax.random.permutation(rng, count)
    heavy_load, common = portions_of(count, rows * top, most, lean, True), portions_of(count, rows * top, most, lean, False)
    places = jnp.arange(count)

    def named(sizes, turn):
        used = int((sizes > 0).sum())
        fixed = max(1, used // 4)
        passed = fixed + (places - fixed + turn * (used - fixed)) % max(1, count - fixed)
        return jnp.zeros((count,), jnp.int32).at[order[jnp.where(places < fixed, places, passed)]].set(jnp.asarray(sizes, jnp.int32))

    sizes = jnp.where(number % 4 == 0, named(heavy_load, number // 4), named(common, number - number // 4 - 1))
    mixed = jax.random.permutation(jax.random.fold_in(own, 3), count)
    giver, sink = mixed[0:count // 2 * 2:2], mixed[1:count // 2 * 2:2]
    margin = jnp.minimum(sizes[giver] - 1, most - sizes[sink]) // 2
    margin = jnp.where((giver == order[0]) | (sink == order[0]) | (sizes[sink] == 0), 0, jnp.maximum(margin, 0))
    passed = jax.random.randint(jax.random.fold_in(own, 4), (count // 2,), 0, 1 << 20) % (margin + 1)
    sizes = sizes.at[giver].add(-passed).at[sink].add(passed)
    labels = jnp.searchsorted(jnp.cumsum(sizes), jnp.arange(rows * top), side="right").astype(jnp.int32)
    listing = labels.reshape(top, rows).T
    listing = listing[jax.random.permutation(jax.random.fold_in(own, 1), rows)]
    turn = jax.random.randint(jax.random.fold_in(own, 2), (rows, 1), 0, top)
    return jnp.take_along_axis(listing, (jnp.arange(top)[None, :] + turn) % top, axis=1)


def portions_of(count, total, limit, lean, full):
    portions = [(1 << 20) // math.isqrt(standing ** lean) + 1 for standing in range(1, count + 1)]
    largest = limit if full else min(limit, max(-(-total // count), total * portions[0] // sum(portions)))
    least = 1 if total - largest >= count - 1 else 0
    given, surplus = [largest] + [least] * (count - 1), total - largest - least * (count - 1)
    while surplus > 0:
        candidates = [i for i in range(1, count) if given[i] < largest] or [i for i in range(1, count) if given[i] < limit]
        pool, left = sum([portions[i] for i in candidates]), surplus
        for i in candidates:
            more = min(limit - given[i], max(1, left * portions[i] // pool), surplus)
            given[i] = given[i] + more
            surplus = surplus - more
    return np.array(given)


def noise(rng, extent, width, most, cuts=(), held_as=jnp.bfloat16):
    level = shard_levels(rng, extent, cuts, -0.22, 0.18) if cuts else 1.0
    array = jax.random.normal(rng, extent, jnp.float32) * width * level
    return jnp.minimum(jnp.maximum(array, -most), most).astype(held_as)


def setup_inputs(seed: int = 0) -> dict:
    splits = jax.random.split(jax.random.key(seed), 14)
    pool_in = noise(splits[0], (MIX_TOK, DP), 1.0, 6.0, ((0, 32),))
    pool_weight = noise(splits[1], (4, GROUP, GROUP), GROUP ** -0.5, 0.375)
    pool_gain = jnp.clip(1.0 + 0.18 * jax.random.normal(splits[2], (DP,), jnp.float32), 0.1, 1.9)
    out_weight = noise(splits[3], (DP, D), DP ** -0.5, 0.1875, ((0, 8),))
    mix_gain = jnp.clip(1.0 + 0.18 * jax.random.normal(splits[4], (D,), jnp.float32), 0.1, 1.9)
    expert_in = noise(splits[5], (MOE_TOK, D), 1.0, 6.0, ((0, 4),))
    routes_keys = jax.random.split(jax.random.fold_in(splits[6], 1), MOE_TOK // SUB)
    routes_turns = jax.random.permutation(jax.random.fold_in(splits[6], 3), MOE_TOK // SUB)
    routes = jax.vmap(lambda own, number: deal_out(jax.random.fold_in(splits[6], 2), own, number, SUB, EXPERTS, TOPK, CAP, 2))(routes_keys, routes_turns).reshape((MOE_TOK, TOPK))
    route_weight = jnp.clip(jnp.exp(math.log(1.0) - 2.3025851 * jax.random.uniform(splits[7], (MOE_TOK, TOPK), jnp.float32) ** shard_levels(splits[7], (MOE_TOK, TOPK), ((0, 4),), -0.2, 0.2)), 0.1, 1.0)
    pre_gain = jnp.clip(1.0 + 0.18 * jax.random.normal(splits[8], (D,), jnp.float32), 0.1, 1.9)
    gate_weight = noise(splits[9], (EXPERTS, D, FF), (3.0 * D ** -0.5), 0.39648438, ((0, 4), (2, 8)))
    up_weight = noise(splits[10], (EXPERTS, D, FF), (3.0 * D ** -0.5), 0.39648438, ((0, 4), (2, 8)))
    down_weight = noise(splits[11], (EXPERTS, FF, D), FF ** -0.5, 0.09375, ((0, 4), (1, 8)))
    post_gain = jnp.clip(1.0 + 0.18 * jax.random.normal(splits[12], (D,), jnp.float32), 0.1, 1.9)
    return {"pool_in": pool_in, "pool_weight": pool_weight, "pool_gain": pool_gain, "out_weight": out_weight, "mix_gain": mix_gain, "expert_in": expert_in, "routes": routes, "route_weight": route_weight, "pre_gain": pre_gain, "gate_weight": gate_weight, "up_weight": up_weight, "down_weight": down_weight, "post_gain": post_gain}


WINDOWS = (2, 4, 8, 16)
EPS = 1e-06
LIMIT = 7.0
ALPHA = 1.702

def rms_scale(values, gain):
    mean_square = lax.optimization_barrier(jnp.mean(values * values, axis=-1, keepdims=True))
    return values * lax.rsqrt(mean_square + EPS) * gain.astype(jnp.float32)

def trailing_pool(padded, first_pos, rows):
    group = padded.shape[1] // 4
    position = first_pos + jnp.arange(rows, dtype=jnp.int32)
    pieces = []
    for which, window in enumerate(WINDOWS):
        channels = padded[:, which * group:(which + 1) * group]
        running = channels[16:16 + rows]
        for reach in range(2, window + 1):
            running = running + channels[17 - reach:17 - reach + rows]
        count = jnp.minimum(position + 1, window).astype(jnp.float32)[:, None]
        pieces.append(running / count)
    pooled = jnp.concatenate(pieces, axis=1)
    return (pooled - padded[16:]).astype(jnp.bfloat16)

def selection(block_routes, experts, capacity):
    flat = block_routes.reshape(-1)
    onehot = (flat[:, None] == jnp.arange(experts, dtype=jnp.int32)[None, :]).astype(jnp.int32)
    earlier = jnp.cumsum(onehot, axis=0) - onehot
    rank = lax.optimization_barrier(jnp.sum(earlier * onehot, axis=1))
    slots = (flat * capacity + rank).reshape(block_routes.shape)
    return (slots[:, :, None] == jnp.arange(experts * capacity, dtype=jnp.int32)[None, None, :]).astype(jnp.bfloat16)

def clamped_unit(gate, up):
    gate = jnp.minimum(gate, LIMIT)
    up = jnp.clip(up, -LIMIT, LIMIT)
    return (up + 1.0) * gate * jax.nn.sigmoid(ALPHA * gate)

def expert_rows(rows, gate_w, up_w, down_w):
    gate = jnp.dot(rows, gate_w, preferred_element_type=jnp.float32)
    up = jnp.dot(rows, up_w, preferred_element_type=jnp.float32)
    hidden = clamped_unit(gate, up).astype(jnp.bfloat16)
    parts = hidden.reshape(rows.shape[0], N_TP, FF // N_TP).astype(jnp.float32)
    slices = down_w.reshape(N_TP, FF // N_TP, D).astype(jnp.float32)
    partial_value = jnp.einsum('rtf,tfd->rtd', parts, slices).astype(jnp.bfloat16)
    partial_value = lax.optimization_barrier(partial_value)
    return lax.optimization_barrier(jnp.sum(partial_value.astype(jnp.float32), axis=1)).astype(jnp.bfloat16)

def reference(pool_in, pool_weight, pool_gain, out_weight, mix_gain, expert_in, routes, route_weight, pre_gain, gate_weight, up_weight, down_weight, post_gain):
    rows = pool_in.shape[0]
    padded = jnp.concatenate([jnp.zeros((16, pool_in.shape[1]), jnp.float32), pool_in.astype(jnp.float32)], axis=0)
    diff = trailing_pool(padded, jnp.int32(0), rows)
    grouped = diff.reshape(rows, 4, GROUP).astype(jnp.float32)
    mixed = jnp.einsum('sgc,gcd->sgd', grouped, pool_weight.astype(jnp.float32))
    mixed = (mixed.reshape(rows, DP) * pool_gain.astype(jnp.float32)).astype(jnp.bfloat16)
    projected = jnp.dot(mixed, out_weight, preferred_element_type=jnp.float32)
    mix_out = rms_scale(projected, mix_gain).astype(jnp.bfloat16)
    normed = rms_scale(expert_in.astype(jnp.float32), pre_gain).astype(jnp.bfloat16)
    blocks = routes.shape[0] // SUB
    picks = jax.vmap(lambda block: selection(block, EXPERTS, CAP))(routes.reshape(blocks, SUB, TOPK)).astype(jnp.float32)
    token_picks = lax.optimization_barrier(jnp.sum(picks, axis=2))
    buffers = jnp.einsum('bts,btd->bsd', token_picks, normed.reshape(blocks, SUB, D).astype(jnp.float32)).astype(jnp.bfloat16)
    gathered = buffers.reshape(blocks, EXPERTS, CAP, D).transpose(1, 0, 2, 3).reshape(EXPERTS, blocks * CAP, D)
    outputs = lax.map(lambda operands: expert_rows(*operands), (gathered, gate_weight, up_weight, down_weight))
    back = outputs.reshape(EXPERTS, blocks, CAP, D).transpose(1, 0, 2, 3).reshape(blocks, EXPERTS * CAP, D).astype(jnp.float32)
    per_route = jnp.einsum('btks,bsd->btkd', picks, back)
    weights = route_weight.reshape(blocks, SUB, TOPK).astype(jnp.float32)
    combined = lax.optimization_barrier(jnp.sum(per_route * weights[..., None], axis=2)).reshape(blocks * SUB, D)
    expert_out = rms_scale(combined, post_gain).astype(jnp.bfloat16)
    return (mix_out, expert_out)
```

```python
import jax
import jax.numpy as jnp
from jax import lax
from jax.experimental import pallas as pl
from jax.experimental.pallas import tpu as pltpu
from jax.sharding import PartitionSpec as P

WINDOWS = (2, 4, 8, 16)
EPS = 1e-06
LIMIT = 7.0
ALPHA = 1.702
CORES = 2


def shifted(block, axis, distance):
    devices = range(lax.axis_size(axis))
    route = [(i - distance, i) for i in devices if i - distance in devices]
    return lax.ppermute(block, axis, route)


def moved(block, target):
    eps, tps = lax.axis_size("ep"), lax.axis_size("tp")
    route = []
    for e in range(eps):
        for t in range(tps):
            te, tt = target(e, t)
            route.append((e * tps + t, te * tps + tt))
    return lax.ppermute(block, ("ep", "tp"), route)


def to_core(block):
    return moved(block, lambda e, t: (e, t ^ 1))


def to_group(block, mask):
    return moved(block, lambda e, t: (e ^ mask, t))


def to_chip(block, step):
    chips = lax.axis_size("tp") // CORES
    return moved(block, lambda e, t: (e, (t // CORES + step) % chips * CORES + t % CORES))


def rms_scale(values, gain):
    mean_square = jnp.mean(values * values, axis=-1, keepdims=True)
    return values * lax.rsqrt(mean_square + EPS) * gain


def trailing_pool(padded, first_pos, rows):
    group = padded.shape[1] // 4
    position = first_pos + jnp.arange(rows, dtype=jnp.int32)
    pieces = []
    for which, window in enumerate(WINDOWS):
        channels = padded[:, which * group : (which + 1) * group]
        running = channels[16 : 16 + rows]
        for reach in range(2, window + 1):
            running = running + channels[17 - reach : 17 - reach + rows]
        count = jnp.minimum(position + 1, window).astype(jnp.float32)[:, None]
        pieces.append(running / count)
    pooled = jnp.concatenate(pieces, axis=1)
    return (pooled - padded[16:]).astype(jnp.bfloat16)


def selection(block_routes, experts, capacity):
    flat = block_routes.reshape(-1)
    onehot = (flat[:, None] == jnp.arange(experts, dtype=jnp.int32)[None, :]).astype(jnp.int32)
    earlier = jnp.cumsum(onehot, axis=0) - onehot
    rank = jnp.sum(earlier * onehot, axis=1)
    slots = (flat * capacity + rank).reshape(block_routes.shape)
    return (
        slots[:, :, None] == jnp.arange(experts * capacity, dtype=jnp.int32)[None, None, :]
    ).astype(jnp.bfloat16)


def clamped_unit(gate, up):
    gate = jnp.minimum(gate, LIMIT)
    up = jnp.clip(up, -LIMIT, LIMIT)
    return (up + 1.0) * gate * jax.nn.sigmoid(ALPHA * gate)


def hidden_rows(arrived, gate_weight, up_weight):
    gate = jnp.einsum("necd,edf->necf", arrived, gate_weight, preferred_element_type=jnp.float32)
    up = jnp.einsum("necd,edf->necf", arrived, up_weight, preferred_element_type=jnp.float32)
    return clamped_unit(gate, up).astype(jnp.bfloat16)


def routed_experts(
    expert_in, routes, route_weight, pre_gain, gate_weight, up_weight, down_weight, post_gain
):
    width = expert_in.shape[1]
    ep_count = lax.axis_size("ep")
    tp_count = lax.axis_size("tp")
    tp_place = lax.axis_index("tp")
    local_experts = gate_weight.shape[0]
    experts = local_experts * ep_count
    tokens_here, choose = routes.shape
    block_tokens = tokens_here // tp_count
    capacity = 2 * block_tokens * choose // experts
    block_routes = lax.dynamic_slice_in_dim(routes, tp_place * block_tokens, block_tokens, 0)
    block_rows = lax.dynamic_slice_in_dim(expert_in, tp_place * block_tokens, block_tokens, 0)
    normed = rms_scale(block_rows.astype(jnp.float32), pre_gain).astype(jnp.bfloat16)
    own_picks = selection(block_routes, experts, capacity)
    buffer = jnp.einsum(
        "ts,td->sd", jnp.sum(own_picks, axis=1), normed, preferred_element_type=jnp.float32
    ).astype(jnp.bfloat16)
    buffer = buffer.reshape(ep_count, local_experts, capacity, width)
    arrived = lax.all_to_all(buffer, "ep", split_axis=0, concat_axis=0, tiled=True)
    hidden_all = hidden_rows(
        lax.all_gather(arrived, "tp", axis=0, tiled=True), gate_weight, up_weight
    )
    summed = lax.psum_scatter(
        jnp.einsum(
            "necf,efd->necd", hidden_all, down_weight, preferred_element_type=jnp.float32
        ).astype(jnp.bfloat16),
        "tp",
        scatter_dimension=0,
        tiled=True,
    )
    returned = lax.all_to_all(summed, "ep", split_axis=0, concat_axis=0, tiled=True)
    returned = returned.reshape(experts * capacity, width)
    per_route = jnp.einsum("tks,sd->tkd", own_picks, returned, preferred_element_type=jnp.float32)
    weights = lax.dynamic_slice_in_dim(route_weight, tp_place * block_tokens, block_tokens, 0)
    combined = jnp.sum(per_route * weights[:, :, None], axis=1)
    return rms_scale(combined, post_gain).astype(jnp.bfloat16)


def expert_kernel(
    first_ref, mine_ref, other_ref, gain_ref, share_ref, gate_ref, up_ref, down_ref,
    mine_out, other_out, normed, total,
):
    expert, tile = pl.program_id(0), pl.program_id(1)
    half = mine_ref.shape[0]

    @pl.when((expert == 0) & (tile == 0))
    def _():
        for source, start in ((mine_ref, 0), (other_ref, half)):
            values = source[...].astype(jnp.float32)
            normed[start : start + half, :] = rms_scale(values, gain_ref[...]).astype(jnp.bfloat16)
        total[...] = jnp.zeros_like(total)

    rows = normed[...]
    gate = jnp.dot(rows, gate_ref[0], preferred_element_type=jnp.float32)
    up = jnp.dot(rows, up_ref[0], preferred_element_type=jnp.float32)
    shares = jnp.transpose(share_ref[...])
    lanes = lax.broadcasted_iota(jnp.int32, shares.shape, 1)
    share = jnp.sum(jnp.where(lanes == first_ref[0] + expert, shares, 0.0), axis=1, keepdims=True)
    hidden = (clamped_unit(gate, up) * share).astype(jnp.bfloat16)
    total[...] += jnp.dot(hidden, down_ref[0], preferred_element_type=jnp.float32)

    @pl.when((expert == pl.num_programs(0) - 1) & (tile == pl.num_programs(1) - 1))
    def _():
        mine_out[...] = total[:half, :].astype(jnp.bfloat16)
        other_out[...] = total[half:, :].astype(jnp.bfloat16)


def expert_partial(first, mine, other, gain, share, gate_weight, up_weight, down_weight):
    half, width = mine.shape
    local, _, units = gate_weight.shape
    tile = min(256, units)
    whole = lambda shape: pl.BlockSpec(shape, lambda e, f, *_: (0,) * len(shape))
    spec = pltpu.PrefetchScalarGridSpec(
        num_scalar_prefetch=1,
        grid=(local, units // tile),
        in_specs=[
            whole((half, width)),
            whole((half, width)),
            whole((1, width)),
            whole(share.shape),
            pl.BlockSpec((1, width, tile), lambda e, f, *_: (e, 0, f)),
            pl.BlockSpec((1, width, tile), lambda e, f, *_: (e, 0, f)),
            pl.BlockSpec((1, tile, width), lambda e, f, *_: (e, f, 0)),
        ],
        out_specs=[whole((half, width)), whole((half, width))],
        scratch_shapes=[
            pltpu.VMEM((2 * half, width), jnp.bfloat16),
            pltpu.VMEM((2 * half, width), jnp.float32),
        ],
    )
    flops = 2 * (2 * half) * width * (local * units) * 3
    return pl.pallas_call(
        expert_kernel,
        grid_spec=spec,
        out_shape=[jax.ShapeDtypeStruct((half, width), jnp.bfloat16)] * 2,
        compiler_params=pltpu.CompilerParams(
            dimension_semantics=("arbitrary", "arbitrary"), vmem_limit_bytes=40 << 20
        ),
        cost_estimate=pl.CostEstimate(
            flops=flops,
            bytes_accessed=3 * local * width * units * 2,
            transcendentals=2 * half * local * units,
        ),
        name="experts",
    )(first, mine, other, gain.reshape(1, width), share, gate_weight, up_weight, down_weight)


def split_cores(array, core):
    chips = lax.axis_size("tp") // CORES
    parts = array.reshape(chips, CORES, -1, array.shape[1])
    take = lambda which: lax.dynamic_index_in_dim(parts, which, 1, keepdims=False).reshape(
        -1, array.shape[1]
    )
    return take(core), take(1 - core)


def dense_experts(
    expert_in, routes, route_weight, pre_gain, gate_weight, up_weight, down_weight, post_gain
):
    width = expert_in.shape[1]
    groups = lax.axis_size("ep")
    chips = lax.axis_size("tp") // CORES
    local = gate_weight.shape[0]
    experts = local * groups
    place = lax.axis_index("tp")
    core, chip = place % CORES, place // CORES
    mine, other = split_cores(expert_in, core)
    routes_in = jnp.concatenate(split_cores(routes, core), axis=0)
    weight_in = jnp.concatenate(split_cores(route_weight, core), axis=0)
    numbers = jnp.arange(-(-experts // 8) * 8, dtype=jnp.int32)
    share = jnp.sum(
        jnp.where(routes_in.T[None] == numbers[:, None, None], weight_in.T[None], 0.0), axis=1
    )
    masks = range(1, groups)
    mine_from = {0: mine} | {m: to_group(mine, m) for m in masks}
    share_from = {0: share} | {m: to_group(share, m) for m in masks}
    other_from = {0: other} | {m: to_core(mine_from[m]) for m in masks}
    first = (lax.axis_index("ep") * local).astype(jnp.int32).reshape(1)
    sums = {}
    for m in range(groups):
        kept, sent = expert_partial(
            first, mine_from[m], other_from[m], pre_gain, share_from[m],
            gate_weight, up_weight, down_weight,
        )
        sums[m] = kept.astype(jnp.float32) + to_core(sent).astype(jnp.float32)
    total = sums[0]
    for m in masks:
        total = total + to_group(sums[m].astype(jnp.bfloat16), m).astype(jnp.float32)
    parts = total.reshape(chips, -1, width)
    outgoing = parts.astype(jnp.bfloat16)
    combined = lax.dynamic_index_in_dim(parts, chip, 0, keepdims=False)
    for step in range(1, chips):
        piece = lax.dynamic_index_in_dim(outgoing, (chip + step) % chips, 0, keepdims=False)
        combined = combined + to_chip(piece, step).astype(jnp.float32)
    return rms_scale(combined, post_gain).astype(jnp.bfloat16)


def project_kernel(order_ref, mixed_ref, gain_ref, *refs):
    weights, out_ref = refs[:-1], refs[-1]
    pairs = len(weights) // 2
    total = None
    for pair in range(pairs):
        left = jnp.concatenate(
            [mixed_ref[order_ref[2 * pair]], mixed_ref[order_ref[2 * pair + 1]]], axis=1
        )
        right = jnp.concatenate([weights[2 * pair][...], weights[2 * pair + 1][...]], axis=0)
        part = jnp.dot(left, right, preferred_element_type=jnp.float32)
        total = part if total is None else total + part
    out_ref[...] = rms_scale(total, gain_ref[...]).astype(jnp.bfloat16)


def project(order, mixed, gain, weights):
    shards, rows, depth = mixed.shape
    width = weights[0].shape[1]
    tile = min(256, rows)
    spec = pltpu.PrefetchScalarGridSpec(
        num_scalar_prefetch=1,
        grid=(rows // tile,),
        in_specs=[
            pl.BlockSpec((shards, tile, depth), lambda i, *_: (0, i, 0)),
            pl.BlockSpec((1, width), lambda i, *_: (0, 0)),
        ]
        + [pl.BlockSpec((depth, width), lambda i, *_: (0, 0))] * shards,
        out_specs=pl.BlockSpec((tile, width), lambda i, *_: (i, 0)),
    )
    return pl.pallas_call(
        project_kernel,
        grid_spec=spec,
        out_shape=jax.ShapeDtypeStruct((rows, width), jnp.bfloat16),
        compiler_params=pltpu.CompilerParams(vmem_limit_bytes=40 << 20),
        cost_estimate=pl.CostEstimate(
            flops=2 * rows * shards * depth * width,
            bytes_accessed=2 * (rows * width + shards * depth * (rows + width)),
            transcendentals=0,
        ),
        name="project",
    )(order, mixed, gain.reshape(1, width), *weights)


def body(
    pool_in,
    pool_weight,
    pool_gain,
    out_weight,
    mix_gain,
    expert_in,
    routes,
    route_weight,
    pre_gain,
    gate_weight,
    up_weight,
    down_weight,
    post_gain,
):
    rows, channels = pool_in.shape
    ep_count, tp_count = lax.axis_size("ep"), lax.axis_size("tp")
    chips = tp_count // CORES
    place = lax.axis_index("tp")
    core, chip = place % CORES, place // CORES
    tokens_here, choose = routes.shape
    block_tokens = tokens_here // tp_count
    capacity = 2 * block_tokens * choose // (gate_weight.shape[0] * ep_count)
    dense = capacity >= block_tokens and ep_count & (ep_count - 1) == 0
    experts = dense_experts if dense else routed_experts
    expert_out = experts(
        expert_in, routes, route_weight, pre_gain, gate_weight, up_weight, down_weight, post_gain
    )
    shards, order = [], []
    for step in range(chips):
        shard = to_chip(out_weight, step) if step else out_weight
        source = (chip - step) % chips * CORES
        shards += [shard, to_core(shard)]
        order += [source + core, source + 1 - core]
    rim = shifted(pool_in[rows - 16 :], ("ep", "tp"), 1)
    padded = jnp.concatenate([rim, pool_in], axis=0).astype(jnp.float32)
    first_pos = (lax.axis_index("ep") * tp_count + place) * rows
    diff = trailing_pool(padded, first_pos, rows)
    mixed = jnp.einsum(
        "sgc,gcd->sgd",
        diff.reshape(rows, 4, channels // 4),
        pool_weight,
        preferred_element_type=jnp.float32,
    )
    mixed = (mixed.reshape(rows, channels) * pool_gain).astype(jnp.bfloat16)
    mixed = mixed.reshape(rows, tp_count, -1).transpose(1, 0, 2)
    mix_out = project(jnp.stack(order).astype(jnp.int32), mixed, mix_gain, shards)
    return (mix_out, expert_out)


def solution(mesh):
    return jax.shard_map(
        body,
        mesh=mesh,
        in_specs=(
            P(("ep", "tp"), None),
            P(),
            P(),
            P("tp", None),
            P(),
            P("ep", None),
            P("ep", None),
            P("ep", None),
            P(),
            P("ep", None, "tp"),
            P("ep", None, "tp"),
            P("ep", "tp", None),
            P(),
        ),
        out_specs=(P(("ep", "tp"), None), P(("ep", "tp"), None)),
        check_vma=False,
    )
```

```python
import jax
import jax.numpy as jnp
from jax import lax
from jax.experimental import pallas as pl
from jax.experimental.pallas import tpu as pltpu
from jax.sharding import PartitionSpec as P


WINDOWS = (2, 4, 8, 16)
EPS = 1e-06
LIMIT = 7.0
ALPHA = 1.702
CORES = 2


def shifted(block, axis, distance):
    devices = range(lax.axis_size(axis))
    route = [(i - distance, i) for i in devices if i - distance in devices]
    return lax.ppermute(block, axis, route)


def moved(block, target):
    eps, tps = lax.axis_size("ep"), lax.axis_size("tp")
    route = []
    for e in range(eps):
        for t in range(tps):
            te, tt = target(e, t)
            route.append((e * tps + t, te * tps + tt))
    return lax.ppermute(block, ("ep", "tp"), route)


def to_core(block):
    return moved(block, lambda e, t: (e, t ^ 1))


def to_group(block, mask):
    return moved(block, lambda e, t: (e ^ mask, t))


def to_chip(block, step):
    chips = lax.axis_size("tp") // CORES
    return moved(block, lambda e, t: (e, (t // CORES + step) % chips * CORES + t % CORES))


def rms_scale(values, gain):
    mean_square = jnp.mean(values * values, axis=-1, keepdims=True)
    return values * lax.rsqrt(mean_square + EPS) * gain


def selection(block_routes, experts, capacity):
    flat = block_routes.reshape(-1)
    onehot = (flat[:, None] == jnp.arange(experts, dtype=jnp.int32)[None, :]).astype(jnp.int32)
    earlier = jnp.cumsum(onehot, axis=0) - onehot
    rank = jnp.sum(earlier * onehot, axis=1)
    slots = (flat * capacity + rank).reshape(block_routes.shape)
    return (
        slots[:, :, None] == jnp.arange(experts * capacity, dtype=jnp.int32)[None, None, :]
    ).astype(jnp.bfloat16)


def clamped_unit(gate, up):
    gate = jnp.minimum(gate, LIMIT)
    up = jnp.clip(up, -LIMIT, LIMIT)
    return (up + 1.0) * gate * jax.nn.sigmoid(ALPHA * gate)


def hidden_rows(arrived, gate_weight, up_weight):
    gate = jnp.einsum("necd,edf->necf", arrived, gate_weight, preferred_element_type=jnp.float32)
    up = jnp.einsum("necd,edf->necf", arrived, up_weight, preferred_element_type=jnp.float32)
    return clamped_unit(gate, up).astype(jnp.bfloat16)


def routed_experts(
    expert_in, routes, route_weight, pre_gain, gate_weight, up_weight, down_weight, post_gain
):
    width = expert_in.shape[1]
    ep_count = lax.axis_size("ep")
    tp_count = lax.axis_size("tp")
    tp_place = lax.axis_index("tp")
    local_experts = gate_weight.shape[0]
    experts = local_experts * ep_count
    tokens_here, choose = routes.shape
    block_tokens = tokens_here // tp_count
    capacity = 2 * block_tokens * choose // experts
    block_routes = lax.dynamic_slice_in_dim(routes, tp_place * block_tokens, block_tokens, 0)
    block_rows = lax.dynamic_slice_in_dim(expert_in, tp_place * block_tokens, block_tokens, 0)
    normed = rms_scale(block_rows.astype(jnp.float32), pre_gain).astype(jnp.bfloat16)
    own_picks = selection(block_routes, experts, capacity)
    buffer = jnp.einsum(
        "ts,td->sd", jnp.sum(own_picks, axis=1), normed, preferred_element_type=jnp.float32
    ).astype(jnp.bfloat16)
    buffer = buffer.reshape(ep_count, local_experts, capacity, width)
    arrived = lax.all_to_all(buffer, "ep", split_axis=0, concat_axis=0, tiled=True)
    hidden_all = hidden_rows(
        lax.all_gather(arrived, "tp", axis=0, tiled=True), gate_weight, up_weight
    )
    summed = lax.psum_scatter(
        jnp.einsum(
            "necf,efd->necd", hidden_all, down_weight, preferred_element_type=jnp.float32
        ).astype(jnp.bfloat16),
        "tp",
        scatter_dimension=0,
        tiled=True,
    )
    returned = lax.all_to_all(summed, "ep", split_axis=0, concat_axis=0, tiled=True)
    returned = returned.reshape(experts * capacity, width)
    per_route = jnp.einsum("tks,sd->tkd", own_picks, returned, preferred_element_type=jnp.float32)
    weights = lax.dynamic_slice_in_dim(route_weight, tp_place * block_tokens, block_tokens, 0)
    combined = jnp.sum(per_route * weights[:, :, None], axis=1)
    return rms_scale(combined, post_gain).astype(jnp.bfloat16)


def seat():
    place = lax.axis_index("tp")
    return lax.div(place, CORES), lax.rem(place, CORES)


VMEM = pl.BlockSpec(memory_space=pltpu.VMEM)


def normed_rows(source, gain):
    return rms_scale(source[...].astype(jnp.float32), gain[...]).astype(jnp.bfloat16)


def fill_hidden(hidden, expert, first, normed, share, gate_weight, up_weight):
    units = gate_weight.shape[1]
    lanes = lax.broadcasted_iota(jnp.int32, share.shape, 1)
    gate = jnp.dot(normed[...], gate_weight[...], preferred_element_type=jnp.float32)
    up = jnp.dot(normed[...], up_weight[...], preferred_element_type=jnp.float32)
    scale = jnp.sum(jnp.where(lanes == first + expert, share, 0.0), axis=1, keepdims=True)
    hidden[:, expert * units : (expert + 1) * units] = (clamped_unit(gate, up) * scale).astype(
        jnp.bfloat16
    )


def store_halves(hidden, down_weight, total, core, outputs):
    result = jnp.dot(hidden[...], down_weight[...], preferred_element_type=jnp.float32)
    total[...] = result.astype(jnp.bfloat16).reshape(total.shape)
    groups = len(outputs) // 2
    chips = total.shape[0] // (CORES * groups)
    block = total.shape[1]
    for group in range(groups):
        for chip in range(chips):
            start = CORES * (group * chips + chip)
            rows_of = slice(chip * block, (chip + 1) * block)
            outputs[2 * group][rows_of, :] = total[start + core]
            outputs[2 * group + 1][rows_of, :] = total[start + 1 - core]


def own_kernel(
    gain_ref, rows_ref, share_ref, gate_in, up_in, down_in,
    kept_ref, sent_ref, gate_ref, up_ref, down_ref, normed, hidden, total, sems,
):
    local, _, units = gate_ref.shape
    first = lax.axis_index("ep") * local
    loads = []
    for expert in range(local):
        loads.append(pltpu.make_async_copy(gate_in.at[expert], gate_ref.at[expert], sems.at[len(loads)]))
        loads.append(pltpu.make_async_copy(up_in.at[expert], up_ref.at[expert], sems.at[len(loads)]))
    for expert in range(local):
        part = pl.ds(expert * units, units)
        loads.append(pltpu.make_async_copy(down_in.at[part], down_ref.at[part], sems.at[len(loads)]))
    for load in loads:
        load.start()
    normed[...] = normed_rows(rows_ref, gain_ref)
    share = jnp.transpose(share_ref[...])
    for expert in range(local):
        loads[2 * expert].wait()
        loads[2 * expert + 1].wait()
        fill_hidden(
            hidden, expert, first, normed, share, gate_ref.at[expert], up_ref.at[expert]
        )
    for load in loads[2 * local :]:
        load.wait()
    store_halves(hidden, down_ref, total, seat()[1], (kept_ref, sent_ref))


def own_partial(rows, share, gain, gate_weight, up_weight, down_weight, block):
    tokens, width = rows.shape
    local, _, units = gate_weight.shape
    half = jax.ShapeDtypeStruct((tokens // 2, width), jnp.bfloat16)
    down_weight = down_weight.reshape(-1, width)
    held = [pltpu.VMEM(w.shape, w.dtype) for w in (gate_weight, up_weight, down_weight)]
    hbm = pl.BlockSpec(memory_space=pltpu.HBM)
    return pl.pallas_call(
        own_kernel,
        in_specs=[VMEM] * 3 + [hbm] * 3,
        out_specs=[VMEM] * 5,
        out_shape=[half, half] + held,
        scratch_shapes=[
            pltpu.VMEM((tokens, width), jnp.bfloat16),
            pltpu.VMEM((tokens, local * units), jnp.bfloat16),
            pltpu.VMEM((tokens // block, block, width), jnp.bfloat16),
            pltpu.SemaphoreType.DMA((3 * local,)),
        ],
        compiler_params=pltpu.CompilerParams(vmem_limit_bytes=10 << 20),
        cost_estimate=pl.CostEstimate(
            flops=6 * tokens * width * local * units,
            bytes_accessed=4 * tokens * width + 6 * local * units * width,
            transcendentals=tokens * local * units,
        ),
        name="own",
    )(
        gain.reshape(1, width), rows, share,
        *(
            pltpu.with_memory_space_constraint(w, pltpu.HBM)
            for w in (gate_weight, up_weight, down_weight)
        ),
    )


def expert_kernel(gain_ref, gate_ref, up_ref, down_ref, *refs, groups):
    inputs, outputs = refs[: 3 * groups], refs[3 * groups : 5 * groups]
    normed, hidden, total = refs[5 * groups :]
    first, core = lax.axis_index("ep") * gate_ref.shape[0], seat()[1]
    half = inputs[0].shape[0]
    shares = []
    for group in range(groups):
        mine_ref, other_ref, share_ref = inputs[3 * group : 3 * group + 3]
        for source, which in ((mine_ref, core), (other_ref, 1 - core)):
            start = pl.multiple_of((2 * group + which) * half, half)
            normed[pl.ds(start, half), :] = normed_rows(source, gain_ref)
        shares.append(jnp.transpose(share_ref[...]))
    share = jnp.concatenate(shares, axis=0)
    for expert in range(gate_ref.shape[0]):
        fill_hidden(hidden, expert, first, normed, share, gate_ref.at[expert], up_ref.at[expert])
    store_halves(hidden, down_ref, total, core, outputs)


def expert_partial(chunks, gain, gate_weight, up_weight, down_weight, block):
    groups = len(chunks)
    half, width = chunks[0][0].shape
    rows = 2 * half * groups
    local, _, units = gate_weight.shape
    inputs = [array for chunk in chunks for array in chunk]
    outputs = pl.pallas_call(
        lambda *refs: expert_kernel(*refs, groups=groups),
        in_specs=[VMEM] * (4 + len(inputs)),
        out_specs=[VMEM] * (2 * groups),
        out_shape=[jax.ShapeDtypeStruct((half, width), jnp.bfloat16)] * (2 * groups),
        scratch_shapes=[
            pltpu.VMEM((rows, width), jnp.bfloat16),
            pltpu.VMEM((rows, local * units), jnp.bfloat16),
            pltpu.VMEM((rows // block, block, width), jnp.bfloat16),
        ],
        compiler_params=pltpu.CompilerParams(vmem_limit_bytes=16 << 20),
        cost_estimate=pl.CostEstimate(
            flops=6 * rows * width * local * units,
            bytes_accessed=4 * rows * width,
            transcendentals=rows * local * units,
        ),
        name="experts",
    )(gain.reshape(1, width), gate_weight, up_weight, down_weight, *inputs)
    return [(outputs[2 * g], outputs[2 * g + 1]) for g in range(groups)]


def spread_kernel(early_ref, late_ref, own_ref, *out_refs):
    chips = early_ref.shape[0]
    for step in range(chips):
        at = lax.rem(seat()[0] + step, chips)
        part = early_ref[at] + late_ref[at].astype(jnp.float32)
        if step:
            out_refs[step - 1][...] = part.astype(jnp.bfloat16)
        else:
            own_ref[...] = part


def spread(early, late):
    chips, block, width = early.shape
    return pl.pallas_call(
        spread_kernel,
        in_specs=[VMEM, VMEM],
        out_specs=[VMEM] * chips,
        out_shape=[jax.ShapeDtypeStruct((block, width), jnp.float32)]
        + [jax.ShapeDtypeStruct((block, width), jnp.bfloat16)] * (chips - 1),
        cost_estimate=pl.CostEstimate(
            flops=early.size, bytes_accessed=8 * early.size, transcendentals=0
        ),
        compiler_params=pltpu.CompilerParams(vmem_limit_bytes=4 << 20),
        name="spread",
    )(early, late)


def finish_kernel(gain_ref, own_ref, *refs):
    total = own_ref[...]
    for ref in refs[:-1]:
        total = total + ref[...].astype(jnp.float32)
    refs[-1][...] = rms_scale(total, gain_ref[...]).astype(jnp.bfloat16)


def finish(gain, own, parts):
    return pl.pallas_call(
        finish_kernel,
        in_specs=[VMEM] * (2 + len(parts)),
        out_specs=VMEM,
        out_shape=jax.ShapeDtypeStruct(own.shape, jnp.bfloat16),
        compiler_params=pltpu.CompilerParams(vmem_limit_bytes=4 << 20),
        name="finish",
    )(gain.reshape(1, -1), own, *parts)


def dense_experts(
    expert_in, routes, route_weight, pre_gain, gate_weight, up_weight, down_weight, post_gain
):
    tokens, width = expert_in.shape
    groups = lax.axis_size("ep")
    chips = lax.axis_size("tp") // CORES
    block = tokens // lax.axis_size("tp")
    local = gate_weight.shape[0]
    experts = local * groups
    place = lax.axis_index("tp")
    core = place % CORES
    masks = range(1, groups)
    mine = lax.dynamic_slice_in_dim(expert_in, core * (tokens // CORES), tokens // CORES, 0)
    mine_from = {}
    for m in masks:
        mine_from[m] = to_group(mine, m)
    numbers = jnp.arange(-(-experts // 8) * 8, dtype=jnp.int32)
    share = jnp.sum(
        jnp.where(routes.T[None] == numbers[:, None, None], route_weight.T[None], 0.0), axis=1
    )
    share_from = {}
    for m in masks:
        share_from[m] = to_group(share, m)
    kept, sent, *held = own_partial(
        expert_in, share, pre_gain, gate_weight, up_weight, down_weight, block
    )
    weights = (pre_gain, *held, block)
    early = kept.astype(jnp.float32) + to_core(sent).astype(jnp.float32)
    near = [m for m in masks if m & (m - 1) == 0]
    far = [m for m in masks if m & (m - 1) != 0]
    returned = {}
    for batch in (near, far):
        chunks = []
        for m in batch:
            chunks.append((mine_from[m], to_core(mine_from[m]), share_from[m]))
        results = expert_partial(chunks, *weights)
        for m, (kept, sent) in zip(batch, results):
            partner = to_core(sent)
            joined = (kept.astype(jnp.float32) + partner.astype(jnp.float32)).astype(jnp.bfloat16)
            returned[m] = to_group(joined, m)
    for m in masks[:-1]:
        early = early + returned[m].astype(jnp.float32)
    early = lax.optimization_barrier(early)
    own, *pieces = spread(
        early.reshape(chips, block, width),
        returned[masks[-1]].reshape(chips, block, width),
    )
    parts = []
    for step in range(1, chips):
        parts.append(to_chip(pieces[step - 1], step))
    return finish(post_gain, own, parts)


def mix_kernel(rim_ref, rows_ref, weight_ref, gain_ref, out_ref):
    rows = rows_ref.shape[0]
    group = rows_ref.shape[1] // len(WINDOWS)
    spare = rim_ref.shape[0]
    device = lax.axis_index("ep") * lax.axis_size("tp") + lax.axis_index("tp")
    position = device * rows + lax.broadcasted_iota(jnp.int32, (rows, 1), 0)
    for which, window in enumerate(WINDOWS):
        cols = slice(which * group, (which + 1) * group)
        values = jnp.concatenate([rim_ref[:, cols], rows_ref[:, cols]], axis=0)
        values = values.astype(jnp.float32)
        running, reach = values, 1
        while reach < window:
            running = running + pltpu.roll(running, reach, 0)
            reach *= 2
        count = jnp.minimum(position + 1, window).astype(jnp.float32)
        diff = running[spare:] / count - values[spare:]
        mixed = jnp.dot(
            diff.astype(jnp.bfloat16), weight_ref[which], preferred_element_type=jnp.float32
        )
        out_ref[:, cols] = (mixed * gain_ref[:, cols]).astype(jnp.bfloat16)


def mix(rim, rows, weight, gain):
    return pl.pallas_call(
        mix_kernel,
        in_specs=[VMEM] * 4,
        out_specs=VMEM,
        out_shape=jax.ShapeDtypeStruct(rows.shape, jnp.bfloat16),
        compiler_params=pltpu.CompilerParams(vmem_limit_bytes=6 << 20),
        cost_estimate=pl.CostEstimate(
            flops=2 * rows.size * weight.shape[1],
            bytes_accessed=4 * rows.size,
            transcendentals=0,
        ),
        name="mix",
    )(rim, rows, weight, gain.reshape(1, -1))


def project_kernel(mixed_ref, gain_ref, *refs):
    weights, out_ref, joined = refs[:-2], refs[-2], refs[-1]

    @pl.when(pl.program_id(0) == 0)
    def _():
        depth = weights[0].shape[0]
        chip, core = seat()
        chips = len(weights) // CORES
        for k, weight in enumerate(weights):
            source = lax.rem(chip + chips - k // CORES, chips) * CORES
            shard = source + (core if k % CORES == 0 else 1 - core)
            joined[pl.ds(pl.multiple_of(shard * depth, depth), depth), :] = weight[...]

    total = jnp.dot(mixed_ref[...], joined[...], preferred_element_type=jnp.float32)
    out_ref[...] = rms_scale(total, gain_ref[...]).astype(jnp.bfloat16)


def project(mixed, gain, weights):
    rows, depth = mixed.shape
    width = weights[0].shape[1]
    tile = min(256, rows)
    return pl.pallas_call(
        project_kernel,
        grid=(rows // tile,),
        in_specs=[
            pl.BlockSpec((tile, depth), lambda i: (i, 0)),
            pl.BlockSpec((1, width), lambda i: (0, 0)),
        ]
        + [VMEM] * len(weights),
        out_specs=pl.BlockSpec((tile, width), lambda i: (i, 0)),
        out_shape=jax.ShapeDtypeStruct((rows, width), jnp.bfloat16),
        scratch_shapes=[pltpu.VMEM((depth, width), jnp.bfloat16)],
        compiler_params=pltpu.CompilerParams(vmem_limit_bytes=18 << 20),
        cost_estimate=pl.CostEstimate(
            flops=2 * rows * depth * width,
            bytes_accessed=2 * (rows * width + depth * (rows + width)),
            transcendentals=0,
        ),
        name="project",
    )(mixed, gain.reshape(1, width), *weights)


def step(
    pool_in,
    pool_weight,
    pool_gain,
    out_weight,
    mix_gain,
    expert_in,
    routes,
    route_weight,
    pre_gain,
    gate_weight,
    up_weight,
    down_weight,
    post_gain,
):
    rows, _ = pool_in.shape
    ep_count, tp_count = lax.axis_size("ep"), lax.axis_size("tp")
    chips = tp_count // CORES
    tokens_here, choose = routes.shape
    block_tokens = tokens_here // tp_count
    capacity = 2 * block_tokens * choose // (gate_weight.shape[0] * ep_count)
    dense = capacity >= block_tokens and ep_count & (ep_count - 1) == 0
    experts = dense_experts if dense else routed_experts
    rim = shifted(pool_in[rows - 16 :], ("ep", "tp"), 1)
    expert_out = experts(
        expert_in, routes, route_weight, pre_gain, gate_weight, up_weight, down_weight, post_gain
    )
    shards = []
    for step in range(chips):
        shard = to_chip(out_weight, step) if step else out_weight
        shards += [shard, to_core(shard)]
    mixed = mix(rim, pool_in, pool_weight, pool_gain)
    mix_out = project(mixed, mix_gain, shards)
    return (mix_out, expert_out)


def solution(mesh):
    return jax.shard_map(
        step,
        mesh=mesh,
        in_specs=(
            P(("ep", "tp"), None),
            P(),
            P(),
            P("tp", None),
            P(),
            P("ep", None),
            P("ep", None),
            P("ep", None),
            P(),
            P("ep", None, "tp"),
            P("ep", None, "tp"),
            P("ep", "tp", None),
            P(),
        ),
        out_specs=(P(("ep", "tp"), None), P(("ep", "tp"), None)),
        check_vma=False,
    )
```

```python
import jax
import jax.numpy as jnp
from jax import lax
from jax.experimental import pallas as pl
from jax.experimental.pallas import tpu as pltpu
from jax.sharding import PartitionSpec as P


WINDOWS = (2, 4, 8, 16)
EPS = 1e-06
LIMIT = 7.0
ALPHA = 1.702
CORES = 2


def shifted(block, axis, distance):
    devices = range(lax.axis_size(axis))
    route = [(i - distance, i) for i in devices if i - distance in devices]
    return lax.ppermute(block, axis, route)


def moved(block, target):
    eps, tps = lax.axis_size("ep"), lax.axis_size("tp")
    route = []
    for e in range(eps):
        for t in range(tps):
            te, tt = target(e, t)
            route.append((e * tps + t, te * tps + tt))
    return lax.ppermute(block, ("ep", "tp"), route)


def to_core(block):
    return moved(block, lambda e, t: (e, t ^ 1))


def to_group(block, mask):
    return moved(block, lambda e, t: (e ^ mask, t))


def paired(chips):
    return chips & (chips - 1) == 0


def to_chip(block, step):
    chips = lax.axis_size("tp") // CORES
    target = (lambda z: z ^ step) if paired(chips) else (lambda z: (z + step) % chips)
    return moved(block, lambda e, t: (e, target(t // CORES) * CORES + t % CORES))


def chip_after(chip, step, chips):
    return lax.bitwise_xor(chip, step) if paired(chips) else lax.rem(chip + step, chips)


def chip_before(chip, step, chips):
    return lax.bitwise_xor(chip, step) if paired(chips) else lax.rem(chip + chips - step, chips)


def rms_scale(values, gain):
    mean_square = jnp.mean(values * values, axis=-1, keepdims=True)
    return values * lax.rsqrt(mean_square + EPS) * gain


def selection(block_routes, experts, capacity):
    flat = block_routes.reshape(-1)
    onehot = (flat[:, None] == jnp.arange(experts, dtype=jnp.int32)[None, :]).astype(jnp.int32)
    earlier = jnp.cumsum(onehot, axis=0) - onehot
    rank = jnp.sum(earlier * onehot, axis=1)
    slots = (flat * capacity + rank).reshape(block_routes.shape)
    return (
        slots[:, :, None] == jnp.arange(experts * capacity, dtype=jnp.int32)[None, None, :]
    ).astype(jnp.bfloat16)


def clamped_unit(gate, up):
    gate = jnp.minimum(gate, LIMIT)
    up = jnp.clip(up, -LIMIT, LIMIT)
    return (up + 1.0) * gate * jax.nn.sigmoid(ALPHA * gate)


def hidden_rows(arrived, gate_weight, up_weight):
    gate = jnp.einsum("necd,edf->necf", arrived, gate_weight, preferred_element_type=jnp.float32)
    up = jnp.einsum("necd,edf->necf", arrived, up_weight, preferred_element_type=jnp.float32)
    return clamped_unit(gate, up).astype(jnp.bfloat16)


def routed_experts(
    expert_in, routes, route_weight, pre_gain, gate_weight, up_weight, down_weight, post_gain
):
    width = expert_in.shape[1]
    ep_count = lax.axis_size("ep")
    tp_count = lax.axis_size("tp")
    tp_place = lax.axis_index("tp")
    local_experts = gate_weight.shape[0]
    experts = local_experts * ep_count
    tokens_here, choose = routes.shape
    block_tokens = tokens_here // tp_count
    capacity = 2 * block_tokens * choose // experts
    block_routes = lax.dynamic_slice_in_dim(routes, tp_place * block_tokens, block_tokens, 0)
    block_rows = lax.dynamic_slice_in_dim(expert_in, tp_place * block_tokens, block_tokens, 0)
    normed = rms_scale(block_rows.astype(jnp.float32), pre_gain).astype(jnp.bfloat16)
    own_picks = selection(block_routes, experts, capacity)
    buffer = jnp.einsum(
        "ts,td->sd", jnp.sum(own_picks, axis=1), normed, preferred_element_type=jnp.float32
    ).astype(jnp.bfloat16)
    buffer = buffer.reshape(ep_count, local_experts, capacity, width)
    arrived = lax.all_to_all(buffer, "ep", split_axis=0, concat_axis=0, tiled=True)
    hidden_all = hidden_rows(
        lax.all_gather(arrived, "tp", axis=0, tiled=True), gate_weight, up_weight
    )
    summed = lax.psum_scatter(
        jnp.einsum(
            "necf,efd->necd", hidden_all, down_weight, preferred_element_type=jnp.float32
        ).astype(jnp.bfloat16),
        "tp",
        scatter_dimension=0,
        tiled=True,
    )
    returned = lax.all_to_all(summed, "ep", split_axis=0, concat_axis=0, tiled=True)
    returned = returned.reshape(experts * capacity, width)
    per_route = jnp.einsum("tks,sd->tkd", own_picks, returned, preferred_element_type=jnp.float32)
    weights = lax.dynamic_slice_in_dim(route_weight, tp_place * block_tokens, block_tokens, 0)
    combined = jnp.sum(per_route * weights[:, :, None], axis=1)
    return rms_scale(combined, post_gain).astype(jnp.bfloat16)


def seat():
    place = lax.axis_index("tp")
    return lax.div(place, CORES), lax.rem(place, CORES)


VMEM = pl.BlockSpec(memory_space=pltpu.VMEM)
HBM = pl.BlockSpec(memory_space=pltpu.HBM)


def normed_rows(source, gain):
    return rms_scale(source[...].astype(jnp.float32), gain[...]).astype(jnp.bfloat16)


def share_of(message, expert, tokens):
    start = pl.multiple_of(expert * tokens, tokens)
    notes = message[tokens // CORES :, pl.ds(start, tokens)].astype(jnp.float32)
    notes = jnp.transpose(notes)
    return notes[:, 0:1] + notes[:, 1:2]


def fill_hidden(hidden, expert, scale, normed, gate_weight, up_weight):
    units = gate_weight.shape[1]
    gate = jnp.dot(normed[...], gate_weight[...], preferred_element_type=jnp.float32)
    up = jnp.dot(normed[...], up_weight[...], preferred_element_type=jnp.float32)
    hidden[:, expert * units : (expert + 1) * units] = (clamped_unit(gate, up) * scale).astype(
        jnp.bfloat16
    )


def store_halves(hidden, down_weight, total, core, outputs):
    result = jnp.dot(hidden[...], down_weight[...], preferred_element_type=jnp.float32)
    total[...] = result.astype(jnp.bfloat16).reshape(total.shape)
    groups = len(outputs) // 2
    chips = total.shape[0] // (CORES * groups)
    block = total.shape[1]
    for group in range(groups):
        for chip in range(chips):
            start = CORES * (group * chips + chip)
            rows_of = slice(chip * block, (chip + 1) * block)
            outputs[2 * group][rows_of, :] = total[start + core]
            outputs[2 * group + 1][rows_of, :] = total[start + 1 - core]


def start_all(pairs, sems):
    copies = [
        pltpu.make_async_copy(source, target, sems.at[k])
        for k, (source, target) in enumerate(pairs)
    ]
    for copy in copies:
        copy.start()
    return copies


def from_hbm(*arrays):
    return [pltpu.with_memory_space_constraint(array, pltpu.HBM) for array in arrays]


def pack_kernel(rows_ref, routes_in, weight_in, message_ref, routes_ref, weight_ref, sems):
    half = rows_ref.shape[0] // CORES
    tokens = routes_ref.shape[1]
    experts = message_ref.shape[1] // tokens
    start = pl.multiple_of(seat()[1] * half, half)
    copies = start_all(
        [
            (routes_in, routes_ref),
            (weight_in, weight_ref),
            (rows_ref.at[pl.ds(start, half)], message_ref.at[pl.ds(0, half)]),
        ],
        sems,
    )
    copies[0].wait()
    copies[1].wait()
    notes = message_ref.shape[0] - half
    line = lax.broadcasted_iota(jnp.int32, (notes, tokens), 0)
    for expert in range(experts):
        share = jnp.sum(
            jnp.where(routes_ref[...] == expert, weight_ref[...], 0.0), axis=0, keepdims=True
        )
        coarse = share.astype(jnp.bfloat16).astype(jnp.float32)
        both = jnp.where(line == 0, coarse, jnp.where(line == 1, share - coarse, 0.0))
        message_ref[half:, expert * tokens : (expert + 1) * tokens] = both.astype(jnp.bfloat16)
    copies[2].wait()


def pack(rows, routes, route_weight):
    tokens, width = rows.shape
    choose = routes.shape[1]
    return pl.pallas_call(
        pack_kernel,
        in_specs=[HBM] * 3,
        out_specs=VMEM,
        out_shape=jax.ShapeDtypeStruct((tokens // CORES + 8, width), rows.dtype),
        scratch_shapes=[
            pltpu.VMEM((choose, tokens), jnp.int32),
            pltpu.VMEM((choose, tokens), jnp.float32),
            pltpu.SemaphoreType.DMA((3,)),
        ],
        compiler_params=pltpu.CompilerParams(vmem_limit_bytes=2 << 20),
        name="pack",
    )(*from_hbm(rows, routes.T, route_weight.T))


def own_kernel(
    gain_in, rows_in, gate_in, up_in, down_in, message_ref,
    kept_ref, sent_ref, gate_ref, up_ref, down_ref,
    gain_ref, rows_ref, normed, hidden, total, sems,
):
    local, _, units = gate_ref.shape
    tokens = rows_ref.shape[0]
    first = lax.axis_index("ep") * local
    pairs = [(rows_in, rows_ref), (gain_in, gain_ref)]
    for expert in range(local):
        pairs.append((gate_in.at[expert], gate_ref.at[expert]))
        pairs.append((up_in.at[expert], up_ref.at[expert]))
    for expert in range(local):
        part = pl.ds(expert * units, units)
        pairs.append((down_in.at[part], down_ref.at[part]))
    copies = start_all(pairs, sems)
    copies[0].wait()
    copies[1].wait()
    normed[...] = normed_rows(rows_ref, gain_ref)
    for expert in range(local):
        copies[2 + 2 * expert].wait()
        copies[3 + 2 * expert].wait()
        scale = share_of(message_ref, first + expert, tokens)
        fill_hidden(hidden, expert, scale, normed, gate_ref.at[expert], up_ref.at[expert])
    for copy in copies[2 + 2 * local :]:
        copy.wait()
    store_halves(hidden, down_ref, total, seat()[1], (kept_ref, sent_ref))


def own_partial(rows, message, gain, gate_weight, up_weight, down_weight, block):
    tokens, width = rows.shape
    local, _, units = gate_weight.shape
    half = jax.ShapeDtypeStruct((tokens // 2, width), jnp.bfloat16)
    held = [pltpu.VMEM(w.shape, w.dtype) for w in (gate_weight, up_weight, down_weight)]
    return pl.pallas_call(
        own_kernel,
        in_specs=[HBM] * 5 + [VMEM],
        out_specs=[VMEM] * 5,
        out_shape=[half, half] + held,
        scratch_shapes=[
            pltpu.VMEM((1, width), jnp.float32),
            pltpu.VMEM((tokens, width), rows.dtype),
            pltpu.VMEM((tokens, width), jnp.bfloat16),
            pltpu.VMEM((tokens, local * units), jnp.bfloat16),
            pltpu.VMEM((tokens // block, block, width), jnp.bfloat16),
            pltpu.SemaphoreType.DMA((2 + 3 * local,)),
        ],
        compiler_params=pltpu.CompilerParams(vmem_limit_bytes=10 << 20),
        cost_estimate=pl.CostEstimate(
            flops=6 * tokens * width * local * units,
            bytes_accessed=4 * tokens * width + 6 * local * units * width,
            transcendentals=tokens * local * units,
        ),
        name="own",
    )(*from_hbm(gain.reshape(1, width), rows, gate_weight, up_weight, down_weight), message)


def expert_kernel(gain_ref, gate_ref, up_ref, down_ref, *refs, groups):
    inputs, outputs = refs[: 2 * groups], refs[2 * groups : 4 * groups]
    normed, hidden, total = refs[4 * groups :]
    first, core = lax.axis_index("ep") * gate_ref.shape[0], seat()[1]
    half = normed.shape[0] // (2 * groups)
    for group in range(groups):
        mine_ref, other_ref = inputs[2 * group : 2 * group + 2]
        for source, which in ((mine_ref, core), (other_ref, 1 - core)):
            start = pl.multiple_of((2 * group + which) * half, half)
            normed[pl.ds(start, half), :] = normed_rows(source.at[:half], gain_ref)
    for expert in range(gate_ref.shape[0]):
        shares = [share_of(ref, first + expert, 2 * half) for ref in inputs[::2]]
        scale = jnp.concatenate(shares, axis=0)
        fill_hidden(hidden, expert, scale, normed, gate_ref.at[expert], up_ref.at[expert])
    store_halves(hidden, down_ref, total, core, outputs)


def expert_partial(chunks, gain, gate_weight, up_weight, down_weight, block):
    groups = len(chunks)
    half, width = chunks[0][0].shape
    half -= 8
    rows = 2 * half * groups
    local, _, units = gate_weight.shape
    inputs = [array for chunk in chunks for array in chunk]
    outputs = pl.pallas_call(
        lambda *refs: expert_kernel(*refs, groups=groups),
        in_specs=[VMEM] * (4 + len(inputs)),
        out_specs=[VMEM] * (2 * groups),
        out_shape=[jax.ShapeDtypeStruct((half, width), jnp.bfloat16)] * (2 * groups),
        scratch_shapes=[
            pltpu.VMEM((rows, width), jnp.bfloat16),
            pltpu.VMEM((rows, local * units), jnp.bfloat16),
            pltpu.VMEM((rows // block, block, width), jnp.bfloat16),
        ],
        compiler_params=pltpu.CompilerParams(vmem_limit_bytes=16 << 20),
        cost_estimate=pl.CostEstimate(
            flops=6 * rows * width * local * units,
            bytes_accessed=4 * rows * width,
            transcendentals=rows * local * units,
        ),
        name="experts",
    )(gain.reshape(1, width), gate_weight, up_weight, down_weight, *inputs)
    return [(outputs[2 * g], outputs[2 * g + 1]) for g in range(groups)]


def spread_kernel(early_ref, late_ref, own_ref, *out_refs):
    chips = early_ref.shape[0]
    for step in range(chips):
        at = chip_after(seat()[0], step, chips)
        part = early_ref[at] + late_ref[at].astype(jnp.float32)
        if step:
            out_refs[step - 1][...] = part.astype(jnp.bfloat16)
        else:
            own_ref[...] = part


def spread(early, late):
    chips, block, width = early.shape
    return pl.pallas_call(
        spread_kernel,
        in_specs=[VMEM, VMEM],
        out_specs=[VMEM] * chips,
        out_shape=[jax.ShapeDtypeStruct((block, width), jnp.float32)]
        + [jax.ShapeDtypeStruct((block, width), jnp.bfloat16)] * (chips - 1),
        cost_estimate=pl.CostEstimate(
            flops=early.size, bytes_accessed=8 * early.size, transcendentals=0
        ),
        compiler_params=pltpu.CompilerParams(vmem_limit_bytes=4 << 20),
        name="spread",
    )(early, late)


def finish_kernel(gain_ref, own_ref, *refs):
    total = own_ref[...]
    for ref in refs[:-1]:
        total = total + ref[...].astype(jnp.float32)
    refs[-1][...] = rms_scale(total, gain_ref[...]).astype(jnp.bfloat16)


def finish(gain, own, parts):
    return pl.pallas_call(
        finish_kernel,
        in_specs=[VMEM] * (2 + len(parts)),
        out_specs=VMEM,
        out_shape=jax.ShapeDtypeStruct(own.shape, jnp.bfloat16),
        compiler_params=pltpu.CompilerParams(vmem_limit_bytes=4 << 20),
        name="finish",
    )(gain.reshape(1, -1), own, *parts)


def dense_experts(
    expert_in, routes, route_weight, pre_gain, gate_weight, up_weight, down_weight, post_gain
):
    tokens, width = expert_in.shape
    groups = lax.axis_size("ep")
    chips = lax.axis_size("tp") // CORES
    block = tokens // lax.axis_size("tp")
    masks = range(1, groups)
    message = pack(expert_in, routes, route_weight)
    mine_from = {}
    for m in masks:
        mine_from[m] = to_group(message, m)
    weights = (pre_gain, gate_weight, up_weight, down_weight.reshape(-1, width), block)
    kept, sent, *held = own_partial(expert_in, message, *weights)
    weights = (pre_gain, *held, block)
    early = kept.astype(jnp.float32) + to_core(sent).astype(jnp.float32)
    near = [m for m in masks if m & (m - 1) == 0]
    far = [m for m in masks if m & (m - 1) != 0]
    returned = {}
    for batch in (near, far):
        chunks = []
        for m in batch:
            chunks.append((mine_from[m], to_core(mine_from[m])))
        results = expert_partial(chunks, *weights)
        for m, (kept, sent) in zip(batch, results):
            partner = to_core(sent)
            joined = (kept.astype(jnp.float32) + partner.astype(jnp.float32)).astype(jnp.bfloat16)
            returned[m] = to_group(joined, m)
    for m in masks[:-1]:
        early = early + returned[m].astype(jnp.float32)
    early = lax.optimization_barrier(early)
    own, *pieces = spread(
        early.reshape(chips, block, width),
        returned[masks[-1]].reshape(chips, block, width),
    )
    parts = []
    for step in range(1, chips):
        parts.append(to_chip(pieces[step - 1], step))
    return finish(post_gain, own, parts)


def mix_kernel(rim_ref, rows_ref, weight_ref, gain_ref, out_ref):
    rows = rows_ref.shape[0]
    group = rows_ref.shape[1] // len(WINDOWS)
    spare = rim_ref.shape[0]
    device = lax.axis_index("ep") * lax.axis_size("tp") + lax.axis_index("tp")
    position = device * rows + lax.broadcasted_iota(jnp.int32, (rows, 1), 0)
    for which, window in enumerate(WINDOWS):
        cols = slice(which * group, (which + 1) * group)
        values = jnp.concatenate([rim_ref[:, cols], rows_ref[:, cols]], axis=0)
        values = values.astype(jnp.float32)
        running, reach = values, 1
        while reach < window:
            running = running + pltpu.roll(running, reach, 0)
            reach *= 2
        count = jnp.minimum(position + 1, window).astype(jnp.float32)
        diff = running[spare:] / count - values[spare:]
        mixed = jnp.dot(
            diff.astype(jnp.bfloat16), weight_ref[which], preferred_element_type=jnp.float32
        )
        out_ref[:, cols] = (mixed * gain_ref[:, cols]).astype(jnp.bfloat16)


def mix(rim, rows, weight, gain):
    return pl.pallas_call(
        mix_kernel,
        in_specs=[VMEM] * 4,
        out_specs=VMEM,
        out_shape=jax.ShapeDtypeStruct(rows.shape, jnp.bfloat16),
        compiler_params=pltpu.CompilerParams(vmem_limit_bytes=6 << 20),
        cost_estimate=pl.CostEstimate(
            flops=2 * rows.size * weight.shape[1],
            bytes_accessed=4 * rows.size,
            transcendentals=0,
        ),
        name="mix",
    )(rim, rows, weight, gain.reshape(1, -1))


def project_kernel(mixed_ref, gain_ref, *refs):
    weights, out_ref, joined = refs[:-2], refs[-2], refs[-1]

    @pl.when(pl.program_id(0) == 0)
    def _():
        depth = weights[0].shape[0]
        chip, core = seat()
        chips = len(weights) // CORES
        for k, weight in enumerate(weights):
            source = chip_before(chip, k // CORES, chips) * CORES
            shard = source + (core if k % CORES == 0 else 1 - core)
            joined[pl.ds(pl.multiple_of(shard * depth, depth), depth), :] = weight[...]

    total = jnp.dot(mixed_ref[...], joined[...], preferred_element_type=jnp.float32)
    out_ref[...] = rms_scale(total, gain_ref[...]).astype(jnp.bfloat16)


def project(mixed, gain, weights):
    rows, depth = mixed.shape
    width = weights[0].shape[1]
    tile = min(256, rows)
    return pl.pallas_call(
        project_kernel,
        grid=(rows // tile,),
        in_specs=[
            pl.BlockSpec((tile, depth), lambda i: (i, 0)),
            pl.BlockSpec((1, width), lambda i: (0, 0)),
        ]
        + [VMEM] * len(weights),
        out_specs=pl.BlockSpec((tile, width), lambda i: (i, 0)),
        out_shape=jax.ShapeDtypeStruct((rows, width), jnp.bfloat16),
        scratch_shapes=[pltpu.VMEM((depth, width), jnp.bfloat16)],
        compiler_params=pltpu.CompilerParams(vmem_limit_bytes=18 << 20),
        cost_estimate=pl.CostEstimate(
            flops=2 * rows * depth * width,
            bytes_accessed=2 * (rows * width + depth * (rows + width)),
            transcendentals=0,
        ),
        name="project",
    )(mixed, gain.reshape(1, width), *weights)


def step(
    pool_in,
    pool_weight,
    pool_gain,
    out_weight,
    mix_gain,
    expert_in,
    routes,
    route_weight,
    pre_gain,
    gate_weight,
    up_weight,
    down_weight,
    post_gain,
):
    rows, _ = pool_in.shape
    ep_count, tp_count = lax.axis_size("ep"), lax.axis_size("tp")
    chips = tp_count // CORES
    tokens_here, choose = routes.shape
    block_tokens = tokens_here // tp_count
    capacity = 2 * block_tokens * choose // (gate_weight.shape[0] * ep_count)
    experts_in_all = gate_weight.shape[0] * ep_count
    dense = capacity >= block_tokens and ep_count & (ep_count - 1) == 0
    dense = dense and experts_in_all * tokens_here <= expert_in.shape[1]
    experts = dense_experts if dense else routed_experts
    rim = shifted(pool_in[rows - 16 :], ("ep", "tp"), 1)
    expert_out = experts(
        expert_in, routes, route_weight, pre_gain, gate_weight, up_weight, down_weight, post_gain
    )
    shards = []
    for step in range(chips):
        shard = to_chip(out_weight, step) if step else out_weight
        shards += [shard, to_core(shard)]
    mixed = mix(rim, pool_in, pool_weight, pool_gain)
    mix_out = project(mixed, mix_gain, shards)
    return (mix_out, expert_out)


def solution(mesh):
    return jax.shard_map(
        step,
        mesh=mesh,
        in_specs=(
            P(("ep", "tp"), None),
            P(),
            P(),
            P("tp", None),
            P(),
            P("ep", None),
            P("ep", None),
            P("ep", None),
            P(),
            P("ep", None, "tp"),
            P("ep", None, "tp"),
            P("ep", "tp", None),
            P(),
        ),
        out_specs=(P(("ep", "tp"), None), P(("ep", "tp"), None)),
        check_vma=False,
    )
```

```python
import jax
import jax.numpy as jnp
from jax import lax
from jax.experimental import pallas as pl
from jax.experimental.pallas import tpu as pltpu
from jax.sharding import PartitionSpec as P


WINDOWS = (2, 4, 8, 16)
EPS = 1e-06
LIMIT = 7.0
ALPHA = 1.702
CORES = 2


def shifted(block, axis, distance):
    devices = range(lax.axis_size(axis))
    route = [(i - distance, i) for i in devices if i - distance in devices]
    return lax.ppermute(block, axis, route)


def moved(block, target):
    eps, tps = lax.axis_size("ep"), lax.axis_size("tp")
    route = []
    for e in range(eps):
        for t in range(tps):
            te, tt = target(e, t)
            route.append((e * tps + t, te * tps + tt))
    return lax.ppermute(block, ("ep", "tp"), route)


def to_core(block):
    return moved(block, lambda e, t: (e, t ^ 1))


def to_group(block, turn):
    masks = (1, 2) if turn == 0 else (2, 1)
    return moved(block, lambda e, t: (e ^ masks[t % CORES], t))


def paired(chips):
    return chips & (chips - 1) == 0


def to_chip(block, step):
    chips = lax.axis_size("tp") // CORES
    target = (lambda z: z ^ step) if paired(chips) else (lambda z: (z + step) % chips)
    return moved(block, lambda e, t: (e, target(t // CORES) * CORES + t % CORES))


def chip_after(chip, step, chips):
    return lax.bitwise_xor(chip, step) if paired(chips) else lax.rem(chip + step, chips)


def chip_before(chip, step, chips):
    return lax.bitwise_xor(chip, step) if paired(chips) else lax.rem(chip + chips - step, chips)


def rms_scale(values, gain):
    mean_square = jnp.mean(values * values, axis=-1, keepdims=True)
    return values * lax.rsqrt(mean_square + EPS) * gain


def selection(block_routes, experts, capacity):
    flat = block_routes.reshape(-1)
    onehot = (flat[:, None] == jnp.arange(experts, dtype=jnp.int32)[None, :]).astype(jnp.int32)
    earlier = jnp.cumsum(onehot, axis=0) - onehot
    rank = jnp.sum(earlier * onehot, axis=1)
    slots = (flat * capacity + rank).reshape(block_routes.shape)
    return (
        slots[:, :, None] == jnp.arange(experts * capacity, dtype=jnp.int32)[None, None, :]
    ).astype(jnp.bfloat16)


def clamped_unit(gate, up):
    gate = jnp.minimum(gate, LIMIT)
    up = jnp.clip(up, -LIMIT, LIMIT)
    return (up + 1.0) * gate * jax.nn.sigmoid(ALPHA * gate)


def hidden_rows(arrived, gate_weight, up_weight):
    gate = jnp.einsum("necd,edf->necf", arrived, gate_weight, preferred_element_type=jnp.float32)
    up = jnp.einsum("necd,edf->necf", arrived, up_weight, preferred_element_type=jnp.float32)
    return clamped_unit(gate, up).astype(jnp.bfloat16)


def routed_experts(
    expert_in, routes, route_weight, pre_gain, gate_weight, up_weight, down_weight, post_gain
):
    width = expert_in.shape[1]
    ep_count = lax.axis_size("ep")
    tp_count = lax.axis_size("tp")
    tp_place = lax.axis_index("tp")
    local_experts = gate_weight.shape[0]
    experts = local_experts * ep_count
    tokens_here, choose = routes.shape
    block_tokens = tokens_here // tp_count
    capacity = 2 * block_tokens * choose // experts
    block_routes = lax.dynamic_slice_in_dim(routes, tp_place * block_tokens, block_tokens, 0)
    block_rows = lax.dynamic_slice_in_dim(expert_in, tp_place * block_tokens, block_tokens, 0)
    normed = rms_scale(block_rows.astype(jnp.float32), pre_gain).astype(jnp.bfloat16)
    own_picks = selection(block_routes, experts, capacity)
    buffer = jnp.einsum(
        "ts,td->sd", jnp.sum(own_picks, axis=1), normed, preferred_element_type=jnp.float32
    ).astype(jnp.bfloat16)
    buffer = buffer.reshape(ep_count, local_experts, capacity, width)
    arrived = lax.all_to_all(buffer, "ep", split_axis=0, concat_axis=0, tiled=True)
    hidden_all = hidden_rows(
        lax.all_gather(arrived, "tp", axis=0, tiled=True), gate_weight, up_weight
    )
    summed = lax.psum_scatter(
        jnp.einsum(
            "necf,efd->necd", hidden_all, down_weight, preferred_element_type=jnp.float32
        ).astype(jnp.bfloat16),
        "tp",
        scatter_dimension=0,
        tiled=True,
    )
    returned = lax.all_to_all(summed, "ep", split_axis=0, concat_axis=0, tiled=True)
    returned = returned.reshape(experts * capacity, width)
    per_route = jnp.einsum("tks,sd->tkd", own_picks, returned, preferred_element_type=jnp.float32)
    weights = lax.dynamic_slice_in_dim(route_weight, tp_place * block_tokens, block_tokens, 0)
    combined = jnp.sum(per_route * weights[:, :, None], axis=1)
    return rms_scale(combined, post_gain).astype(jnp.bfloat16)


def seat():
    place = lax.axis_index("tp")
    return lax.div(place, CORES), lax.rem(place, CORES)


VMEM = pl.BlockSpec(memory_space=pltpu.VMEM)
HBM = pl.BlockSpec(memory_space=pltpu.HBM)


def normed_rows(source, gain):
    return rms_scale(source[...].astype(jnp.float32), gain[...]).astype(jnp.bfloat16)


def share_of(message, expert, tokens):
    start = pl.multiple_of(expert * tokens, tokens)
    notes = message[tokens // CORES :, pl.ds(start, tokens)].astype(jnp.float32)
    notes = jnp.transpose(notes)
    return notes[:, 0:1] + notes[:, 1:2]


def fill_hidden(hidden, expert, scale, normed, gate_weight, up_weight):
    units = gate_weight.shape[1]
    gate = jnp.dot(normed[...], gate_weight[...], preferred_element_type=jnp.float32)
    up = jnp.dot(normed[...], up_weight[...], preferred_element_type=jnp.float32)
    hidden[:, expert * units : (expert + 1) * units] = (clamped_unit(gate, up) * scale).astype(
        jnp.bfloat16
    )


def store_halves(hidden, down_weight, total, core, outputs):
    result = jnp.dot(hidden[...], down_weight[...], preferred_element_type=jnp.float32)
    total[...] = result.astype(jnp.bfloat16).reshape(total.shape)
    groups = len(outputs) // 2
    chips = total.shape[0] // (CORES * groups)
    block = total.shape[1]
    for group in range(groups):
        for chip in range(chips):
            start = CORES * (group * chips + chip)
            rows_of = slice(chip * block, (chip + 1) * block)
            outputs[2 * group][rows_of, :] = total[start + core]
            outputs[2 * group + 1][rows_of, :] = total[start + 1 - core]


def start_all(pairs, sems):
    copies = [
        pltpu.make_async_copy(source, target, sems.at[k])
        for k, (source, target) in enumerate(pairs)
    ]
    for copy in copies:
        copy.start()
    return copies


def from_hbm(*arrays):
    return [pltpu.with_memory_space_constraint(array, pltpu.HBM) for array in arrays]


def pack_kernel(rows_ref, routes_in, weight_in, message_ref, routes_ref, weight_ref, sems):
    half = rows_ref.shape[0] // CORES
    tokens = routes_ref.shape[1]
    experts = message_ref.shape[1] // tokens
    start = pl.multiple_of(seat()[1] * half, half)
    copies = start_all(
        [
            (routes_in, routes_ref),
            (weight_in, weight_ref),
            (rows_ref.at[pl.ds(start, half)], message_ref.at[pl.ds(0, half)]),
        ],
        sems,
    )
    copies[0].wait()
    copies[1].wait()
    notes = message_ref.shape[0] - half
    line = lax.broadcasted_iota(jnp.int32, (notes, tokens), 0)
    for expert in range(experts):
        share = jnp.sum(
            jnp.where(routes_ref[...] == expert, weight_ref[...], 0.0), axis=0, keepdims=True
        )
        coarse = share.astype(jnp.bfloat16).astype(jnp.float32)
        both = jnp.where(line == 0, coarse, jnp.where(line == 1, share - coarse, 0.0))
        message_ref[half:, expert * tokens : (expert + 1) * tokens] = both.astype(jnp.bfloat16)
    copies[2].wait()


def pack(rows, routes, route_weight):
    tokens, width = rows.shape
    choose = routes.shape[1]
    return pl.pallas_call(
        pack_kernel,
        in_specs=[HBM] * 3,
        out_specs=VMEM,
        out_shape=jax.ShapeDtypeStruct((tokens // CORES + 8, width), rows.dtype),
        scratch_shapes=[
            pltpu.VMEM((choose, tokens), jnp.int32),
            pltpu.VMEM((choose, tokens), jnp.float32),
            pltpu.SemaphoreType.DMA((3,)),
        ],
        compiler_params=pltpu.CompilerParams(vmem_limit_bytes=2 << 20),
        name="pack",
    )(*from_hbm(rows, routes.T, route_weight.T))


def own_kernel(
    gain_in, rows_in, gate_in, up_in, down_in, message_ref,
    kept_ref, sent_ref, gate_ref, up_ref, down_ref,
    gain_ref, rows_ref, normed, hidden, total, sems,
):
    local, _, units = gate_ref.shape
    tokens = rows_ref.shape[0]
    first = lax.axis_index("ep") * local
    pairs = [(rows_in, rows_ref), (gain_in, gain_ref)]
    for expert in range(local):
        pairs.append((gate_in.at[expert], gate_ref.at[expert]))
        pairs.append((up_in.at[expert], up_ref.at[expert]))
    for expert in range(local):
        part = pl.ds(expert * units, units)
        pairs.append((down_in.at[part], down_ref.at[part]))
    copies = start_all(pairs, sems)
    copies[0].wait()
    copies[1].wait()
    normed[...] = normed_rows(rows_ref, gain_ref)
    for expert in range(local):
        copies[2 + 2 * expert].wait()
        copies[3 + 2 * expert].wait()
        scale = share_of(message_ref, first + expert, tokens)
        fill_hidden(hidden, expert, scale, normed, gate_ref.at[expert], up_ref.at[expert])
    for copy in copies[2 + 2 * local :]:
        copy.wait()
    store_halves(hidden, down_ref, total, seat()[1], (kept_ref, sent_ref))


def own_partial(rows, message, gain, gate_weight, up_weight, down_weight, block):
    tokens, width = rows.shape
    local, _, units = gate_weight.shape
    half = jax.ShapeDtypeStruct((tokens // 2, width), jnp.bfloat16)
    held = [pltpu.VMEM(w.shape, w.dtype) for w in (gate_weight, up_weight, down_weight)]
    return pl.pallas_call(
        own_kernel,
        in_specs=[HBM] * 5 + [VMEM],
        out_specs=[VMEM] * 5,
        out_shape=[half, half] + held,
        scratch_shapes=[
            pltpu.VMEM((1, width), jnp.float32),
            pltpu.VMEM((tokens, width), rows.dtype),
            pltpu.VMEM((tokens, width), jnp.bfloat16),
            pltpu.VMEM((tokens, local * units), jnp.bfloat16),
            pltpu.VMEM((tokens // block, block, width), jnp.bfloat16),
            pltpu.SemaphoreType.DMA((2 + 3 * local,)),
        ],
        compiler_params=pltpu.CompilerParams(vmem_limit_bytes=10 << 20),
        cost_estimate=pl.CostEstimate(
            flops=6 * tokens * width * local * units,
            bytes_accessed=4 * tokens * width + 6 * local * units * width,
            transcendentals=tokens * local * units,
        ),
        name="own",
    )(*from_hbm(gain.reshape(1, width), rows, gate_weight, up_weight, down_weight), message)


def expert_kernel(gain_ref, gate_ref, up_ref, down_ref, *refs, groups):
    inputs, outputs = refs[: 2 * groups], refs[2 * groups : 4 * groups]
    normed, hidden, total = refs[4 * groups :]
    first, core = lax.axis_index("ep") * gate_ref.shape[0], seat()[1]
    half = normed.shape[0] // (2 * groups)
    for group in range(groups):
        mine_ref, other_ref = inputs[2 * group : 2 * group + 2]
        for source, which in ((mine_ref, core), (other_ref, 1 - core)):
            start = pl.multiple_of((2 * group + which) * half, half)
            normed[pl.ds(start, half), :] = normed_rows(source.at[:half], gain_ref)
    for expert in range(gate_ref.shape[0]):
        shares = [share_of(ref, first + expert, 2 * half) for ref in inputs[::2]]
        scale = jnp.concatenate(shares, axis=0)
        fill_hidden(hidden, expert, scale, normed, gate_ref.at[expert], up_ref.at[expert])
    store_halves(hidden, down_ref, total, core, outputs)


def expert_partial(chunks, gain, gate_weight, up_weight, down_weight, block):
    groups = len(chunks)
    half, width = chunks[0][0].shape
    half -= 8
    rows = 2 * half * groups
    local, _, units = gate_weight.shape
    inputs = [array for chunk in chunks for array in chunk]
    outputs = pl.pallas_call(
        lambda *refs: expert_kernel(*refs, groups=groups),
        in_specs=[VMEM] * (4 + len(inputs)),
        out_specs=[VMEM] * (2 * groups),
        out_shape=[jax.ShapeDtypeStruct((half, width), jnp.bfloat16)] * (2 * groups),
        scratch_shapes=[
            pltpu.VMEM((rows, width), jnp.bfloat16),
            pltpu.VMEM((rows, local * units), jnp.bfloat16),
            pltpu.VMEM((rows // block, block, width), jnp.bfloat16),
        ],
        compiler_params=pltpu.CompilerParams(vmem_limit_bytes=16 << 20),
        cost_estimate=pl.CostEstimate(
            flops=6 * rows * width * local * units,
            bytes_accessed=4 * rows * width,
            transcendentals=rows * local * units,
        ),
        name="experts",
    )(gain.reshape(1, width), gate_weight, up_weight, down_weight, *inputs)
    return [(outputs[2 * g], outputs[2 * g + 1]) for g in range(groups)]


def spread_kernel(early_ref, late_ref, own_ref, *out_refs):
    chips = early_ref.shape[0]
    for step in range(chips):
        at = chip_after(seat()[0], step, chips)
        part = early_ref[at] + late_ref[at].astype(jnp.float32)
        if step:
            out_refs[step - 1][...] = part.astype(jnp.bfloat16)
        else:
            own_ref[...] = part


def spread(early, late):
    chips, block, width = early.shape
    return pl.pallas_call(
        spread_kernel,
        in_specs=[VMEM, VMEM],
        out_specs=[VMEM] * chips,
        out_shape=[jax.ShapeDtypeStruct((block, width), jnp.float32)]
        + [jax.ShapeDtypeStruct((block, width), jnp.bfloat16)] * (chips - 1),
        cost_estimate=pl.CostEstimate(
            flops=early.size, bytes_accessed=8 * early.size, transcendentals=0
        ),
        compiler_params=pltpu.CompilerParams(vmem_limit_bytes=4 << 20),
        name="spread",
    )(early, late)


def finish_kernel(gain_ref, own_ref, *refs):
    total = own_ref[...]
    for ref in refs[:-1]:
        total = total + ref[...].astype(jnp.float32)
    refs[-1][...] = rms_scale(total, gain_ref[...]).astype(jnp.bfloat16)


def finish(gain, own, parts):
    return pl.pallas_call(
        finish_kernel,
        in_specs=[VMEM] * (2 + len(parts)),
        out_specs=VMEM,
        out_shape=jax.ShapeDtypeStruct(own.shape, jnp.bfloat16),
        compiler_params=pltpu.CompilerParams(vmem_limit_bytes=4 << 20),
        name="finish",
    )(gain.reshape(1, -1), own, *parts)


def added(left, right):
    return (left.astype(jnp.float32) + right.astype(jnp.float32)).astype(jnp.bfloat16)


def dense_experts(
    expert_in, routes, route_weight, pre_gain, gate_weight, up_weight, down_weight, post_gain
):
    tokens, width = expert_in.shape
    chips = lax.axis_size("tp") // CORES
    block = tokens // lax.axis_size("tp")
    message = pack(expert_in, routes, route_weight)
    from_a = to_group(message, 0)
    from_b = to_group(message, 1)
    weights = (pre_gain, gate_weight, up_weight, down_weight.reshape(-1, width), block)
    kept, sent, *held = own_partial(expert_in, message, *weights)
    weights = (pre_gain, *held, block)
    early = kept.astype(jnp.float32) + to_core(sent).astype(jnp.float32)
    from_c = to_group(from_a, 1)
    other_b = to_core(from_a)
    other_a = to_core(from_b)
    other_c = to_core(from_c)
    near = expert_partial([(from_a, other_a), (from_b, other_b)], *weights)
    (kept_a, sent_a), (kept_b, sent_b) = near
    back_a = to_core(sent_b)
    back_b = to_core(sent_a)
    joined_a = added(kept_a, back_a)
    joined_b = added(kept_b, back_b)
    near_sum = to_group(joined_a, 0)
    ((kept_c, sent_c),) = expert_partial([(from_c, other_c)], *weights)
    back_c = to_core(sent_c)
    joined_c = added(kept_c, back_c)
    passing = to_group(joined_c, 0)
    passed = added(joined_b, passing)
    far_sum = to_group(passed, 1)
    early = lax.optimization_barrier(early + near_sum.astype(jnp.float32))
    own, *pieces = spread(
        early.reshape(chips, block, width), far_sum.reshape(chips, block, width)
    )
    parts = []
    for step in range(1, chips):
        parts.append(to_chip(pieces[step - 1], step))
    return finish(post_gain, own, parts)


def mix_kernel(rim_ref, rows_ref, weight_ref, gain_ref, out_ref):
    rows = rows_ref.shape[0]
    group = rows_ref.shape[1] // len(WINDOWS)
    spare = rim_ref.shape[0]
    device = lax.axis_index("ep") * lax.axis_size("tp") + lax.axis_index("tp")
    position = device * rows + lax.broadcasted_iota(jnp.int32, (rows, 1), 0)
    for which, window in enumerate(WINDOWS):
        cols = slice(which * group, (which + 1) * group)
        values = jnp.concatenate([rim_ref[:, cols], rows_ref[:, cols]], axis=0)
        values = values.astype(jnp.float32)
        running, reach = values, 1
        while reach < window:
            running = running + pltpu.roll(running, reach, 0)
            reach *= 2
        count = jnp.minimum(position + 1, window).astype(jnp.float32)
        diff = running[spare:] / count - values[spare:]
        mixed = jnp.dot(
            diff.astype(jnp.bfloat16), weight_ref[which], preferred_element_type=jnp.float32
        )
        out_ref[:, cols] = (mixed * gain_ref[:, cols]).astype(jnp.bfloat16)


def mix(rim, rows, weight, gain):
    return pl.pallas_call(
        mix_kernel,
        in_specs=[VMEM] * 4,
        out_specs=VMEM,
        out_shape=jax.ShapeDtypeStruct(rows.shape, jnp.bfloat16),
        compiler_params=pltpu.CompilerParams(vmem_limit_bytes=6 << 20),
        cost_estimate=pl.CostEstimate(
            flops=2 * rows.size * weight.shape[1],
            bytes_accessed=4 * rows.size,
            transcendentals=0,
        ),
        name="mix",
    )(rim, rows, weight, gain.reshape(1, -1))


def project_kernel(mixed_ref, gain_ref, *refs):
    weights, out_ref, joined = refs[:-2], refs[-2], refs[-1]

    @pl.when(pl.program_id(0) == 0)
    def _():
        depth = weights[0].shape[0]
        chip, core = seat()
        chips = len(weights) // CORES
        for k, weight in enumerate(weights):
            source = chip_before(chip, k // CORES, chips) * CORES
            shard = source + (core if k % CORES == 0 else 1 - core)
            joined[pl.ds(pl.multiple_of(shard * depth, depth), depth), :] = weight[...]

    total = jnp.dot(mixed_ref[...], joined[...], preferred_element_type=jnp.float32)
    out_ref[...] = rms_scale(total, gain_ref[...]).astype(jnp.bfloat16)


def project(mixed, gain, weights):
    rows, depth = mixed.shape
    width = weights[0].shape[1]
    tile = min(256, rows)
    return pl.pallas_call(
        project_kernel,
        grid=(rows // tile,),
        in_specs=[
            pl.BlockSpec((tile, depth), lambda i: (i, 0)),
            pl.BlockSpec((1, width), lambda i: (0, 0)),
        ]
        + [VMEM] * len(weights),
        out_specs=pl.BlockSpec((tile, width), lambda i: (i, 0)),
        out_shape=jax.ShapeDtypeStruct((rows, width), jnp.bfloat16),
        scratch_shapes=[pltpu.VMEM((depth, width), jnp.bfloat16)],
        compiler_params=pltpu.CompilerParams(vmem_limit_bytes=18 << 20),
        cost_estimate=pl.CostEstimate(
            flops=2 * rows * depth * width,
            bytes_accessed=2 * (rows * width + depth * (rows + width)),
            transcendentals=0,
        ),
        name="project",
    )(mixed, gain.reshape(1, width), *weights)


def step(
    pool_in,
    pool_weight,
    pool_gain,
    out_weight,
    mix_gain,
    expert_in,
    routes,
    route_weight,
    pre_gain,
    gate_weight,
    up_weight,
    down_weight,
    post_gain,
):
    rows, _ = pool_in.shape
    ep_count, tp_count = lax.axis_size("ep"), lax.axis_size("tp")
    chips = tp_count // CORES
    tokens_here, choose = routes.shape
    block_tokens = tokens_here // tp_count
    capacity = 2 * block_tokens * choose // (gate_weight.shape[0] * ep_count)
    experts_in_all = gate_weight.shape[0] * ep_count
    dense = capacity >= block_tokens and ep_count == 4
    dense = dense and experts_in_all * tokens_here <= expert_in.shape[1]
    experts = dense_experts if dense else routed_experts
    rim = shifted(pool_in[rows - 16 :], ("ep", "tp"), 1)
    expert_out = experts(
        expert_in, routes, route_weight, pre_gain, gate_weight, up_weight, down_weight, post_gain
    )
    shards = []
    for step in range(chips):
        shard = to_chip(out_weight, step) if step else out_weight
        shards += [shard, to_core(shard)]
    mixed = mix(rim, pool_in, pool_weight, pool_gain)
    mix_out = project(mixed, mix_gain, shards)
    return (mix_out, expert_out)


def solution(mesh):
    return jax.shard_map(
        step,
        mesh=mesh,
        in_specs=(
            P(("ep", "tp"), None),
            P(),
            P(),
            P("tp", None),
            P(),
            P("ep", None),
            P("ep", None),
            P("ep", None),
            P(),
            P("ep", None, "tp"),
            P("ep", None, "tp"),
            P("ep", "tp", None),
            P(),
        ),
        out_specs=(P(("ep", "tp"), None), P(("ep", "tp"), None)),
        check_vma=False,
    )
```

```python
import jax
import jax.numpy as jnp
from jax import lax
from jax.experimental import pallas as pl
from jax.experimental.pallas import tpu as pltpu
from jax.sharding import PartitionSpec as P


WINDOWS = (2, 4, 8, 16)
EPS = 1e-06
LIMIT = 7.0
ALPHA = 1.702
CORES = 2
PIECES = 2
REACH = max(WINDOWS)


def to_next(block):
    eps, tps = lax.axis_size("ep"), lax.axis_size("tp")
    return moved(block, lambda e, t: ((e + (t + 1) // tps) % eps, (t + 1) % tps))


def moved(block, target):
    eps, tps = lax.axis_size("ep"), lax.axis_size("tp")
    route = []
    for e in range(eps):
        for t in range(tps):
            te, tt = target(e, t)
            route.append((e * tps + t, te * tps + tt))
    return lax.ppermute(block, ("ep", "tp"), route)


def to_core(block):
    return moved(block, lambda e, t: (e, t ^ 1))


def to_group(block, turn):
    masks = (1, 2) if turn == 0 else (2, 1)
    return moved(block, lambda e, t: (e ^ masks[t % CORES], t))


def paired(chips):
    return chips & (chips - 1) == 0


def to_chip(block, step):
    chips = lax.axis_size("tp") // CORES
    target = (lambda z: z ^ step) if paired(chips) else (lambda z: (z + step) % chips)
    return moved(block, lambda e, t: (e, target(t // CORES) * CORES + t % CORES))


def chip_after(chip, step, chips):
    return lax.bitwise_xor(chip, step) if paired(chips) else lax.rem(chip + step, chips)


def chip_before(chip, step, chips):
    return lax.bitwise_xor(chip, step) if paired(chips) else lax.rem(chip + chips - step, chips)


def rms_scale(values, gain):
    mean_square = jnp.mean(values * values, axis=-1, keepdims=True)
    return values * lax.rsqrt(mean_square + EPS) * gain


def selection(block_routes, experts, capacity):
    flat = block_routes.reshape(-1)
    onehot = (flat[:, None] == jnp.arange(experts, dtype=jnp.int32)[None, :]).astype(jnp.int32)
    earlier = jnp.cumsum(onehot, axis=0) - onehot
    rank = jnp.sum(earlier * onehot, axis=1)
    slots = (flat * capacity + rank).reshape(block_routes.shape)
    return (
        slots[:, :, None] == jnp.arange(experts * capacity, dtype=jnp.int32)[None, None, :]
    ).astype(jnp.bfloat16)


def clamped_unit(gate, up):
    gate = jnp.minimum(gate, LIMIT)
    up = jnp.clip(up, -LIMIT, LIMIT)
    return (up + 1.0) * gate * jax.nn.sigmoid(ALPHA * gate)


def hidden_rows(arrived, gate_weight, up_weight):
    gate = jnp.einsum("necd,edf->necf", arrived, gate_weight, preferred_element_type=jnp.float32)
    up = jnp.einsum("necd,edf->necf", arrived, up_weight, preferred_element_type=jnp.float32)
    return clamped_unit(gate, up).astype(jnp.bfloat16)


def routed_experts(
    expert_in, routes, route_weight, pre_gain, gate_weight, up_weight, down_weight, post_gain
):
    width = expert_in.shape[1]
    ep_count = lax.axis_size("ep")
    tp_count = lax.axis_size("tp")
    tp_place = lax.axis_index("tp")
    local_experts = gate_weight.shape[0]
    experts = local_experts * ep_count
    tokens_here, choose = routes.shape
    block_tokens = tokens_here // tp_count
    capacity = 2 * block_tokens * choose // experts
    block_routes = lax.dynamic_slice_in_dim(routes, tp_place * block_tokens, block_tokens, 0)
    block_rows = lax.dynamic_slice_in_dim(expert_in, tp_place * block_tokens, block_tokens, 0)
    normed = rms_scale(block_rows.astype(jnp.float32), pre_gain).astype(jnp.bfloat16)
    own_picks = selection(block_routes, experts, capacity)
    buffer = jnp.einsum(
        "ts,td->sd", jnp.sum(own_picks, axis=1), normed, preferred_element_type=jnp.float32
    ).astype(jnp.bfloat16)
    buffer = buffer.reshape(ep_count, local_experts, capacity, width)
    arrived = lax.all_to_all(buffer, "ep", split_axis=0, concat_axis=0, tiled=True)
    hidden_all = hidden_rows(
        lax.all_gather(arrived, "tp", axis=0, tiled=True), gate_weight, up_weight
    )
    summed = lax.psum_scatter(
        jnp.einsum(
            "necf,efd->necd", hidden_all, down_weight, preferred_element_type=jnp.float32
        ).astype(jnp.bfloat16),
        "tp",
        scatter_dimension=0,
        tiled=True,
    )
    returned = lax.all_to_all(summed, "ep", split_axis=0, concat_axis=0, tiled=True)
    returned = returned.reshape(experts * capacity, width)
    per_route = jnp.einsum("tks,sd->tkd", own_picks, returned, preferred_element_type=jnp.float32)
    weights = lax.dynamic_slice_in_dim(route_weight, tp_place * block_tokens, block_tokens, 0)
    combined = jnp.sum(per_route * weights[:, :, None], axis=1)
    return rms_scale(combined, post_gain).astype(jnp.bfloat16)


def seat():
    place = lax.axis_index("tp")
    return lax.div(place, CORES), lax.rem(place, CORES)


VMEM = pl.BlockSpec(memory_space=pltpu.VMEM)
HBM = pl.BlockSpec(memory_space=pltpu.HBM)


def normed_rows(source, gain):
    return rms_scale(source[...].astype(jnp.float32), gain[...]).astype(jnp.bfloat16)


def share_of(message, expert, tokens):
    start = pl.multiple_of(expert * tokens, tokens)
    notes = message[tokens // CORES :, pl.ds(start, tokens)].astype(jnp.float32)
    notes = jnp.transpose(notes)
    return notes[:, 0:1] + notes[:, 1:2]


def fill_hidden(hidden, expert, scale, normed, gate_weight, up_weight):
    units = gate_weight.shape[1]
    gate = jnp.dot(normed[...], gate_weight[...], preferred_element_type=jnp.float32)
    up = jnp.dot(normed[...], up_weight[...], preferred_element_type=jnp.float32)
    hidden[:, expert * units : (expert + 1) * units] = (clamped_unit(gate, up) * scale).astype(
        jnp.bfloat16
    )


def store_halves(hidden, down_weight, total, core, outputs):
    result = jnp.dot(hidden[...], down_weight[...], preferred_element_type=jnp.float32)
    total[...] = result.astype(jnp.bfloat16).reshape(total.shape)
    groups = len(outputs) // 2
    chips = total.shape[0] // (CORES * groups)
    block = total.shape[1]
    for group in range(groups):
        for chip in range(chips):
            start = CORES * (group * chips + chip)
            rows_of = slice(chip * block, (chip + 1) * block)
            outputs[2 * group][rows_of, :] = total[start + core]
            outputs[2 * group + 1][rows_of, :] = total[start + 1 - core]


def start_all(pairs, sems):
    copies = [
        pltpu.make_async_copy(source, target, sems.at[k])
        for k, (source, target) in enumerate(pairs)
    ]
    for copy in copies:
        copy.start()
    return copies


def from_hbm(*arrays):
    return [pltpu.with_memory_space_constraint(array, pltpu.HBM) for array in arrays]


def pack_kernel(
    rows_ref, routes_in, weight_in, pool_ref, message_ref, tail_ref, routes_ref, weight_ref, sems
):
    half = rows_ref.shape[0] // CORES
    tokens = routes_ref.shape[1]
    experts = message_ref.shape[1] // tokens
    start = pl.multiple_of(seat()[1] * half, half)
    copies = start_all(
        [
            (routes_in, routes_ref),
            (weight_in, weight_ref),
            (rows_ref.at[pl.ds(start, half)], message_ref.at[pl.ds(0, half)]),
            (pool_ref.at[pl.ds(pool_ref.shape[0] - REACH, REACH)], tail_ref),
        ],
        sems,
    )
    copies[0].wait()
    copies[1].wait()
    notes = message_ref.shape[0] - half
    line = lax.broadcasted_iota(jnp.int32, (notes, tokens), 0)
    for expert in range(experts):
        share = jnp.sum(
            jnp.where(routes_ref[...] == expert, weight_ref[...], 0.0), axis=0, keepdims=True
        )
        coarse = share.astype(jnp.bfloat16).astype(jnp.float32)
        both = jnp.where(line == 0, coarse, jnp.where(line == 1, share - coarse, 0.0))
        message_ref[half:, expert * tokens : (expert + 1) * tokens] = both.astype(jnp.bfloat16)
    copies[2].wait()
    copies[3].wait()


def pack(rows, routes, route_weight, pool_in):
    tokens, width = rows.shape
    choose = routes.shape[1]
    return pl.pallas_call(
        pack_kernel,
        in_specs=[HBM] * 4,
        out_specs=[VMEM] * 2,
        out_shape=[
            jax.ShapeDtypeStruct((tokens // CORES + 8, width), rows.dtype),
            jax.ShapeDtypeStruct((REACH, pool_in.shape[1]), pool_in.dtype),
        ],
        scratch_shapes=[
            pltpu.VMEM((choose, tokens), jnp.int32),
            pltpu.VMEM((choose, tokens), jnp.float32),
            pltpu.SemaphoreType.DMA((4,)),
        ],
        compiler_params=pltpu.CompilerParams(vmem_limit_bytes=2 << 20),
        name="pack",
    )(*from_hbm(rows, routes.T, route_weight.T, pool_in))


def own_kernel(
    gain_in, rows_in, gate_in, up_in, down_in, message_ref,
    kept_ref, sent_ref, gate_ref, up_ref, down_ref,
    gain_ref, rows_ref, normed, hidden, total, sems,
):
    local, _, units = gate_ref.shape
    tokens = rows_ref.shape[0]
    first = lax.axis_index("ep") * local
    pairs = [(rows_in, rows_ref), (gain_in, gain_ref)]
    for expert in range(local):
        pairs.append((gate_in.at[expert], gate_ref.at[expert]))
        pairs.append((up_in.at[expert], up_ref.at[expert]))
    for expert in range(local):
        part = pl.ds(expert * units, units)
        pairs.append((down_in.at[part], down_ref.at[part]))
    copies = start_all(pairs, sems)
    copies[0].wait()
    copies[1].wait()
    normed[...] = normed_rows(rows_ref, gain_ref)
    for expert in range(local):
        copies[2 + 2 * expert].wait()
        copies[3 + 2 * expert].wait()
        scale = share_of(message_ref, first + expert, tokens)
        fill_hidden(hidden, expert, scale, normed, gate_ref.at[expert], up_ref.at[expert])
    for copy in copies[2 + 2 * local :]:
        copy.wait()
    store_halves(hidden, down_ref, total, seat()[1], (kept_ref, sent_ref))


def own_partial(rows, message, gain, gate_weight, up_weight, down_weight, block):
    tokens, width = rows.shape
    local, _, units = gate_weight.shape
    half = jax.ShapeDtypeStruct((tokens // 2, width), jnp.bfloat16)
    held = [pltpu.VMEM(w.shape, w.dtype) for w in (gate_weight, up_weight, down_weight)]
    return pl.pallas_call(
        own_kernel,
        in_specs=[HBM] * 5 + [VMEM],
        out_specs=[VMEM] * 5,
        out_shape=[half, half] + held,
        scratch_shapes=[
            pltpu.VMEM((1, width), jnp.float32),
            pltpu.VMEM((tokens, width), rows.dtype),
            pltpu.VMEM((tokens, width), jnp.bfloat16),
            pltpu.VMEM((tokens, local * units), jnp.bfloat16),
            pltpu.VMEM((tokens // block, block, width), jnp.bfloat16),
            pltpu.SemaphoreType.DMA((2 + 3 * local,)),
        ],
        compiler_params=pltpu.CompilerParams(vmem_limit_bytes=10 << 20),
        cost_estimate=pl.CostEstimate(
            flops=6 * tokens * width * local * units,
            bytes_accessed=4 * tokens * width + 6 * local * units * width,
            transcendentals=tokens * local * units,
        ),
        name="own",
    )(*from_hbm(gain.reshape(1, width), rows, gate_weight, up_weight, down_weight), message)


def expert_kernel(gain_ref, gate_ref, up_ref, down_ref, *refs, groups):
    inputs, outputs = refs[: 2 * groups], refs[2 * groups : 4 * groups]
    normed, hidden, total = refs[4 * groups :]
    first, core = lax.axis_index("ep") * gate_ref.shape[0], seat()[1]
    half = normed.shape[0] // (2 * groups)
    for group in range(groups):
        mine_ref, other_ref = inputs[2 * group : 2 * group + 2]
        for source, which in ((mine_ref, core), (other_ref, 1 - core)):
            start = pl.multiple_of((2 * group + which) * half, half)
            normed[pl.ds(start, half), :] = normed_rows(source.at[:half], gain_ref)
    for expert in range(gate_ref.shape[0]):
        shares = [share_of(ref, first + expert, 2 * half) for ref in inputs[::2]]
        scale = jnp.concatenate(shares, axis=0)
        fill_hidden(hidden, expert, scale, normed, gate_ref.at[expert], up_ref.at[expert])
    store_halves(hidden, down_ref, total, core, outputs)


def expert_partial(chunks, gain, gate_weight, up_weight, down_weight, block):
    groups = len(chunks)
    half, width = chunks[0][0].shape
    half -= 8
    rows = 2 * half * groups
    local, _, units = gate_weight.shape
    inputs = [array for chunk in chunks for array in chunk]
    outputs = pl.pallas_call(
        lambda *refs: expert_kernel(*refs, groups=groups),
        in_specs=[VMEM] * (4 + len(inputs)),
        out_specs=[VMEM] * (2 * groups),
        out_shape=[jax.ShapeDtypeStruct((half, width), jnp.bfloat16)] * (2 * groups),
        scratch_shapes=[
            pltpu.VMEM((rows, width), jnp.bfloat16),
            pltpu.VMEM((rows, local * units), jnp.bfloat16),
            pltpu.VMEM((rows // block, block, width), jnp.bfloat16),
        ],
        compiler_params=pltpu.CompilerParams(vmem_limit_bytes=16 << 20),
        cost_estimate=pl.CostEstimate(
            flops=6 * rows * width * local * units,
            bytes_accessed=4 * rows * width,
            transcendentals=rows * local * units,
        ),
        name="experts",
    )(gain.reshape(1, width), gate_weight, up_weight, down_weight, *inputs)
    return [(outputs[2 * g], outputs[2 * g + 1]) for g in range(groups)]


def spread_kernel(early_ref, late_ref, own_ref, *out_refs, start):
    chips, _, width = late_ref.shape
    for step in range(chips):
        at = chip_after(seat()[0], step, chips)
        part = early_ref[at, :, start : start + width] + late_ref[at].astype(jnp.float32)
        if step:
            out_refs[step - 1][...] = part.astype(jnp.bfloat16)
        else:
            own_ref[...] = part


def spread(early, late, start):
    chips, block, width = late.shape
    return pl.pallas_call(
        lambda *refs: spread_kernel(*refs, start=start),
        in_specs=[VMEM, VMEM],
        out_specs=[VMEM] * chips,
        out_shape=[jax.ShapeDtypeStruct((block, width), jnp.float32)]
        + [jax.ShapeDtypeStruct((block, width), jnp.bfloat16)] * (chips - 1),
        cost_estimate=pl.CostEstimate(
            flops=late.size, bytes_accessed=8 * late.size, transcendentals=0
        ),
        compiler_params=pltpu.CompilerParams(vmem_limit_bytes=4 << 20),
        name="spread",
    )(early, late)


def finish_kernel(gain_ref, *refs):
    inputs, out_ref = refs[:-1], refs[-1]
    each = len(inputs) // PIECES
    totals = []
    for piece in range(PIECES):
        own, *parts = inputs[piece * each : (piece + 1) * each]
        total = own[...]
        for part in parts:
            total = total + part[...].astype(jnp.float32)
        totals.append(total)
    total = jnp.concatenate(totals, axis=1)
    out_ref[...] = rms_scale(total, gain_ref[...]).astype(jnp.bfloat16)


def finish(gain, parts):
    block, width = parts[0].shape
    return pl.pallas_call(
        finish_kernel,
        in_specs=[VMEM] * (1 + len(parts)),
        out_specs=VMEM,
        out_shape=jax.ShapeDtypeStruct((block, width * PIECES), jnp.bfloat16),
        compiler_params=pltpu.CompilerParams(vmem_limit_bytes=4 << 20),
        name="finish",
    )(gain.reshape(1, -1), *parts)


def added(left, right):
    return (left.astype(jnp.float32) + right.astype(jnp.float32)).astype(jnp.bfloat16)


def pass_kernel(held_ref, passing_ref, out_ref, *, start):
    held = held_ref[:, start : start + passing_ref.shape[1]]
    out_ref[...] = added(held, passing_ref[...])


def pass_on(held, passing, start):
    return pl.pallas_call(
        lambda *refs: pass_kernel(*refs, start=start),
        in_specs=[VMEM, VMEM],
        out_specs=VMEM,
        out_shape=jax.ShapeDtypeStruct(passing.shape, passing.dtype),
        compiler_params=pltpu.CompilerParams(vmem_limit_bytes=4 << 20),
        name="pass_on",
    )(held, passing)


def dense_experts(
    message, expert_in, pre_gain, gate_weight, up_weight, down_weight, post_gain
):
    tokens, width = expert_in.shape
    chips = lax.axis_size("tp") // CORES
    block = tokens // lax.axis_size("tp")
    from_a = to_group(message, 0)
    from_b = to_group(message, 1)
    weights = (pre_gain, gate_weight, up_weight, down_weight.reshape(-1, width), block)
    kept, sent, *held = own_partial(expert_in, message, *weights)
    weights = (pre_gain, *held, block)
    early = kept.astype(jnp.float32) + to_core(sent).astype(jnp.float32)
    from_c = to_group(from_a, 1)
    other_b = to_core(from_a)
    other_a = to_core(from_b)
    other_c = to_core(from_c)
    near = expert_partial([(from_a, other_a), (from_b, other_b)], *weights)
    (kept_a, sent_a), (kept_b, sent_b) = near
    back_a = to_core(sent_b)
    back_b = to_core(sent_a)
    joined_a = added(kept_a, back_a)
    joined_b = added(kept_b, back_b)
    near_sum = to_group(joined_a, 0)
    ((kept_c, sent_c),) = expert_partial([(from_c, other_c)], *weights)
    back_c = to_core(sent_c)
    span = width // PIECES
    columns = [slice(piece * span, (piece + 1) * span) for piece in range(PIECES)]
    joined_c = [added(kept_c[:, part], back_c[:, part]) for part in columns]
    passed, late = [], []
    for piece in range(PIECES):
        passing = to_group(joined_c[piece], 0)
        passed.append(pass_on(joined_b, passing, piece * span))
    for piece in range(PIECES):
        late.append(to_group(passed[piece], 1))
    early = lax.optimization_barrier(early + near_sum.astype(jnp.float32))
    early = early.reshape(chips, block, width)
    parts = []
    for piece in range(PIECES):
        own, *pieces = spread(early, late[piece].reshape(chips, block, span), piece * span)
        parts.append(own)
        for step in range(1, chips):
            parts.append(to_chip(pieces[step - 1], step))
    return finish(post_gain, parts)


def mix_kernel(rim_ref, rows_ref, weight_ref, gain_ref, out_ref):
    rows = rows_ref.shape[0]
    group = rows_ref.shape[1] // len(WINDOWS)
    spare = rim_ref.shape[0]
    device = lax.axis_index("ep") * lax.axis_size("tp") + lax.axis_index("tp")
    position = device * rows + lax.broadcasted_iota(jnp.int32, (rows, 1), 0)
    for which, window in enumerate(WINDOWS):
        cols = slice(which * group, (which + 1) * group)
        rim = jnp.where(device == 0, 0.0, rim_ref[:, cols].astype(jnp.float32))
        values = jnp.concatenate([rim, rows_ref[:, cols].astype(jnp.float32)], axis=0)
        running, reach = values, 1
        while reach < window:
            running = running + pltpu.roll(running, reach, 0)
            reach *= 2
        count = jnp.minimum(position + 1, window).astype(jnp.float32)
        diff = running[spare:] / count - values[spare:]
        mixed = jnp.dot(
            diff.astype(jnp.bfloat16), weight_ref[which], preferred_element_type=jnp.float32
        )
        out_ref[:, cols] = (mixed * gain_ref[:, cols]).astype(jnp.bfloat16)


def mix(rim, rows, weight, gain):
    return pl.pallas_call(
        mix_kernel,
        in_specs=[VMEM] * 4,
        out_specs=VMEM,
        out_shape=jax.ShapeDtypeStruct(rows.shape, jnp.bfloat16),
        compiler_params=pltpu.CompilerParams(vmem_limit_bytes=6 << 20),
        cost_estimate=pl.CostEstimate(
            flops=2 * rows.size * weight.shape[1],
            bytes_accessed=4 * rows.size,
            transcendentals=0,
        ),
        name="mix",
    )(rim, rows, weight, gain.reshape(1, -1))


def join_shards(joined, weights, far):
    chip, core = seat()
    chips = 2 * len(weights) // CORES
    depth = weights[0].shape[0]
    base = lax.div(chip, chips // 2)
    base = (1 - base if far else base) * (chips // 2)
    for k, weight in enumerate(weights):
        step = k // CORES + (chips // 2 if far else 0)
        shard = (chip_before(chip, step, chips) - base) * CORES
        shard = shard + (core if k % CORES == 0 else 1 - core)
        joined[pl.ds(pl.multiple_of(shard * depth, depth), depth), :] = weight[...]
    return base * CORES * depth


def near_kernel(mixed_ref, *refs):
    weights, out_ref, joined = refs[:-2], refs[-2], refs[-1]
    span = joined.shape[0]
    start = pl.multiple_of(join_shards(joined, weights, False), span)
    out_ref[...] = jnp.dot(
        mixed_ref[:, pl.ds(start, span)], joined[...], preferred_element_type=jnp.float32
    )


def near_project(mixed, weights):
    rows, depth = mixed.shape
    width = weights[0].shape[1]
    return pl.pallas_call(
        near_kernel,
        in_specs=[VMEM] * (1 + len(weights)),
        out_specs=VMEM,
        out_shape=pltpu.VMEM((rows, width), jnp.float32),
        scratch_shapes=[pltpu.VMEM((depth // 2, width), jnp.bfloat16)],
        compiler_params=pltpu.CompilerParams(vmem_limit_bytes=8 << 20),
        cost_estimate=pl.CostEstimate(
            flops=rows * depth * width, bytes_accessed=4 * rows * width, transcendentals=0
        ),
        name="near",
    )(mixed, *weights)


def project_kernel(mixed_ref, near_ref, gain_ref, *refs):
    weights, out_ref, joined = refs[:-2], refs[-2], refs[-1]
    span, tile = joined.shape[0], out_ref.shape[0]
    row = pl.multiple_of(pl.program_id(0) * tile, tile)

    @pl.when(pl.program_id(0) == 0)
    def _():
        join_shards(joined, weights, True)

    chip, _ = seat()
    chips = 2 * len(weights) // CORES
    start = pl.multiple_of((1 - lax.div(chip, chips // 2)) * span, span)
    total = near_ref[pl.ds(row, tile), :] + jnp.dot(
        mixed_ref[pl.ds(row, tile), pl.ds(start, span)],
        joined[...],
        preferred_element_type=jnp.float32,
    )
    out_ref[...] = rms_scale(total, gain_ref[...]).astype(jnp.bfloat16)


def project(mixed, near, gain, weights):
    rows, depth = mixed.shape
    width = weights[0].shape[1]
    tile = min(256, rows)
    return pl.pallas_call(
        project_kernel,
        grid=(rows // tile,),
        in_specs=[VMEM] * (3 + len(weights)),
        out_specs=pl.BlockSpec((tile, width), lambda i: (i, 0)),
        out_shape=jax.ShapeDtypeStruct((rows, width), jnp.bfloat16),
        scratch_shapes=[pltpu.VMEM((depth // 2, width), jnp.bfloat16)],
        compiler_params=pltpu.CompilerParams(vmem_limit_bytes=8 << 20),
        cost_estimate=pl.CostEstimate(
            flops=rows * depth * width,
            bytes_accessed=6 * rows * width,
            transcendentals=0,
        ),
        name="project",
    )(mixed, near, gain.reshape(1, width), *weights)


def step(
    pool_in,
    pool_weight,
    pool_gain,
    out_weight,
    mix_gain,
    expert_in,
    routes,
    route_weight,
    pre_gain,
    gate_weight,
    up_weight,
    down_weight,
    post_gain,
):
    rows, _ = pool_in.shape
    ep_count, tp_count = lax.axis_size("ep"), lax.axis_size("tp")
    chips = tp_count // CORES
    tokens_here, choose = routes.shape
    block_tokens = tokens_here // tp_count
    capacity = 2 * block_tokens * choose // (gate_weight.shape[0] * ep_count)
    experts_in_all = gate_weight.shape[0] * ep_count
    dense = capacity >= block_tokens and ep_count == 4
    dense = dense and experts_in_all * tokens_here <= expert_in.shape[1]
    tail = pool_in[rows - REACH :]
    if dense:
        message, tail = pack(expert_in, routes, route_weight, pool_in)
    rim = to_next(tail)
    if dense:
        expert_out = dense_experts(
            message, expert_in, pre_gain, gate_weight, up_weight, down_weight, post_gain
        )
    else:
        expert_out = routed_experts(
            expert_in, routes, route_weight, pre_gain, gate_weight, up_weight, down_weight,
            post_gain,
        )
    shards = []
    for step in range(chips):
        shard = to_chip(out_weight, step) if step else out_weight
        shards += [shard, to_core(shard)]
    mixed = mix(rim, pool_in, pool_weight, pool_gain)
    half = len(shards) // 2
    mix_out = project(mixed, near_project(mixed, shards[:half]), mix_gain, shards[half:])
    return (mix_out, expert_out)


def solution(mesh):
    return jax.shard_map(
        step,
        mesh=mesh,
        in_specs=(
            P(("ep", "tp"), None),
            P(),
            P(),
            P("tp", None),
            P(),
            P("ep", None),
            P("ep", None),
            P("ep", None),
            P(),
            P("ep", None, "tp"),
            P("ep", None, "tp"),
            P("ep", "tp", None),
            P(),
        ),
        out_specs=(P(("ep", "tp"), None), P(("ep", "tp"), None)),
        check_vma=False,
    )
```

```python
import jax
import jax.numpy as jnp
from jax import lax
from jax.experimental import pallas as pl
from jax.experimental.pallas import tpu as pltpu
from jax.sharding import PartitionSpec as P


WINDOWS = (2, 4, 8, 16)
EPS = 1e-06
LIMIT = 7.0
ALPHA = 1.702
CORES = 2
PIECES = 2
REACH = max(WINDOWS)


def to_next(block):
    eps, tps = lax.axis_size("ep"), lax.axis_size("tp")
    return moved(block, lambda e, t: ((e + (t + 1) // tps) % eps, (t + 1) % tps))


def moved(block, target):
    eps, tps = lax.axis_size("ep"), lax.axis_size("tp")
    route = []
    for e in range(eps):
        for t in range(tps):
            te, tt = target(e, t)
            route.append((e * tps + t, te * tps + tt))
    return lax.ppermute(block, ("ep", "tp"), route)


def to_core(block):
    return moved(block, lambda e, t: (e, t ^ 1))


def to_group(block, turn):
    masks = (1, 2) if turn == 0 else (2, 1)
    return moved(block, lambda e, t: (e ^ masks[t % CORES], t))


def paired(chips):
    return chips & (chips - 1) == 0


def to_chip(block, step):
    chips = lax.axis_size("tp") // CORES
    target = (lambda z: z ^ step) if paired(chips) else (lambda z: (z + step) % chips)
    return moved(block, lambda e, t: (e, target(t // CORES) * CORES + t % CORES))


def chip_after(chip, step, chips):
    return lax.bitwise_xor(chip, step) if paired(chips) else lax.rem(chip + step, chips)


def chip_before(chip, step, chips):
    return lax.bitwise_xor(chip, step) if paired(chips) else lax.rem(chip + chips - step, chips)


def rms_scale(values, gain):
    mean_square = jnp.mean(values * values, axis=-1, keepdims=True)
    return values * lax.rsqrt(mean_square + EPS) * gain


def selection(block_routes, experts, capacity):
    flat = block_routes.reshape(-1)
    onehot = (flat[:, None] == jnp.arange(experts, dtype=jnp.int32)[None, :]).astype(jnp.int32)
    earlier = jnp.cumsum(onehot, axis=0) - onehot
    rank = jnp.sum(earlier * onehot, axis=1)
    slots = (flat * capacity + rank).reshape(block_routes.shape)
    return (
        slots[:, :, None] == jnp.arange(experts * capacity, dtype=jnp.int32)[None, None, :]
    ).astype(jnp.bfloat16)


def clamped_unit(gate, up):
    gate = jnp.minimum(gate, LIMIT)
    up = jnp.clip(up, -LIMIT, LIMIT)
    return (up + 1.0) * gate * jax.nn.sigmoid(ALPHA * gate)


def hidden_rows(arrived, gate_weight, up_weight):
    gate = jnp.einsum("necd,edf->necf", arrived, gate_weight, preferred_element_type=jnp.float32)
    up = jnp.einsum("necd,edf->necf", arrived, up_weight, preferred_element_type=jnp.float32)
    return clamped_unit(gate, up).astype(jnp.bfloat16)


def routed_experts(
    expert_in, routes, route_weight, pre_gain, gate_weight, up_weight, down_weight, post_gain
):
    width = expert_in.shape[1]
    ep_count = lax.axis_size("ep")
    tp_count = lax.axis_size("tp")
    tp_place = lax.axis_index("tp")
    local_experts = gate_weight.shape[0]
    experts = local_experts * ep_count
    tokens_here, choose = routes.shape
    block_tokens = tokens_here // tp_count
    capacity = 2 * block_tokens * choose // experts
    block_routes = lax.dynamic_slice_in_dim(routes, tp_place * block_tokens, block_tokens, 0)
    block_rows = lax.dynamic_slice_in_dim(expert_in, tp_place * block_tokens, block_tokens, 0)
    normed = rms_scale(block_rows.astype(jnp.float32), pre_gain).astype(jnp.bfloat16)
    own_picks = selection(block_routes, experts, capacity)
    buffer = jnp.einsum(
        "ts,td->sd", jnp.sum(own_picks, axis=1), normed, preferred_element_type=jnp.float32
    ).astype(jnp.bfloat16)
    buffer = buffer.reshape(ep_count, local_experts, capacity, width)
    arrived = lax.all_to_all(buffer, "ep", split_axis=0, concat_axis=0, tiled=True)
    hidden_all = hidden_rows(
        lax.all_gather(arrived, "tp", axis=0, tiled=True), gate_weight, up_weight
    )
    summed = lax.psum_scatter(
        jnp.einsum(
            "necf,efd->necd", hidden_all, down_weight, preferred_element_type=jnp.float32
        ).astype(jnp.bfloat16),
        "tp",
        scatter_dimension=0,
        tiled=True,
    )
    returned = lax.all_to_all(summed, "ep", split_axis=0, concat_axis=0, tiled=True)
    returned = returned.reshape(experts * capacity, width)
    per_route = jnp.einsum("tks,sd->tkd", own_picks, returned, preferred_element_type=jnp.float32)
    weights = lax.dynamic_slice_in_dim(route_weight, tp_place * block_tokens, block_tokens, 0)
    combined = jnp.sum(per_route * weights[:, :, None], axis=1)
    return rms_scale(combined, post_gain).astype(jnp.bfloat16)


def seat():
    place = lax.axis_index("tp")
    return lax.div(place, CORES), lax.rem(place, CORES)


VMEM = pl.BlockSpec(memory_space=pltpu.VMEM)
HBM = pl.BlockSpec(memory_space=pltpu.HBM)


def normed_rows(source, gain):
    return rms_scale(source[...].astype(jnp.float32), gain[...]).astype(jnp.bfloat16)


def share_of(message, expert, tokens):
    start = pl.multiple_of(expert * tokens, tokens)
    notes = message[tokens // CORES :, pl.ds(start, tokens)].astype(jnp.float32)
    notes = jnp.transpose(notes)
    return notes[:, 0:1] + notes[:, 1:2]


def fill_hidden(hidden, expert, scale, normed, gate_weight, up_weight):
    units = gate_weight.shape[1]
    gate = jnp.dot(normed[...], gate_weight[...], preferred_element_type=jnp.float32)
    up = jnp.dot(normed[...], up_weight[...], preferred_element_type=jnp.float32)
    hidden[:, expert * units : (expert + 1) * units] = (clamped_unit(gate, up) * scale).astype(
        jnp.bfloat16
    )


def store_halves(hidden, down_weight, total, core, outputs):
    result = jnp.dot(hidden[...], down_weight[...], preferred_element_type=jnp.float32)
    total[...] = result.astype(jnp.bfloat16).reshape(total.shape)
    groups = len(outputs) // 2
    chips = total.shape[0] // (CORES * groups)
    block = total.shape[1]
    for group in range(groups):
        for chip in range(chips):
            start = CORES * (group * chips + chip)
            rows_of = slice(chip * block, (chip + 1) * block)
            outputs[2 * group][rows_of, :] = total[start + core]
            outputs[2 * group + 1][rows_of, :] = total[start + 1 - core]


def start_all(pairs, sems):
    copies = [
        pltpu.make_async_copy(source, target, sems.at[k])
        for k, (source, target) in enumerate(pairs)
    ]
    for copy in copies:
        copy.start()
    return copies


def from_hbm(*arrays):
    return [pltpu.with_memory_space_constraint(array, pltpu.HBM) for array in arrays]


def pack_kernel(
    rows_in, gain_in, routes_in, weight_in, pool_in,
    message_ref, tail_ref, rows_ref, gain_ref, routes_ref, weight_ref, sems,
):
    half = rows_ref.shape[0]
    tokens = routes_ref.shape[1]
    experts = message_ref.shape[1] // tokens
    start = pl.multiple_of(seat()[1] * half, half)
    copies = start_all(
        [
            (routes_in, routes_ref),
            (weight_in, weight_ref),
            (gain_in, gain_ref),
            (rows_in.at[pl.ds(start, half)], rows_ref),
            (pool_in.at[pl.ds(pool_in.shape[0] - REACH, REACH)], tail_ref),
        ],
        sems,
    )
    copies[0].wait()
    copies[1].wait()
    notes = message_ref.shape[0] - half
    line = lax.broadcasted_iota(jnp.int32, (notes, tokens), 0)
    for expert in range(experts):
        share = jnp.sum(
            jnp.where(routes_ref[...] == expert, weight_ref[...], 0.0), axis=0, keepdims=True
        )
        coarse = share.astype(jnp.bfloat16).astype(jnp.float32)
        both = jnp.where(line == 0, coarse, jnp.where(line == 1, share - coarse, 0.0))
        message_ref[half:, expert * tokens : (expert + 1) * tokens] = both.astype(jnp.bfloat16)
    copies[2].wait()
    copies[3].wait()
    message_ref[:half, :] = normed_rows(rows_ref, gain_ref)
    copies[4].wait()


def pack(rows, gain, routes, route_weight, pool_in):
    tokens, width = rows.shape
    choose = routes.shape[1]
    return pl.pallas_call(
        pack_kernel,
        in_specs=[HBM] * 5,
        out_specs=[VMEM] * 2,
        out_shape=[
            jax.ShapeDtypeStruct((tokens // CORES + 8, width), rows.dtype),
            jax.ShapeDtypeStruct((REACH, pool_in.shape[1]), pool_in.dtype),
        ],
        scratch_shapes=[
            pltpu.VMEM((tokens // CORES, width), rows.dtype),
            pltpu.VMEM((1, width), jnp.float32),
            pltpu.VMEM((choose, tokens), jnp.int32),
            pltpu.VMEM((choose, tokens), jnp.float32),
            pltpu.SemaphoreType.DMA((5,)),
        ],
        compiler_params=pltpu.CompilerParams(vmem_limit_bytes=3 << 20),
        name="pack",
    )(*from_hbm(rows, gain.reshape(1, width), routes.T, route_weight.T, pool_in))


def own_kernel(
    gain_in, rows_in, gate_in, up_in, down_in, message_ref,
    kept_ref, sent_ref, gate_ref, up_ref, down_ref,
    gain_ref, rows_ref, normed, hidden, total, sems,
):
    local, _, units = gate_ref.shape
    tokens = rows_ref.shape[0]
    first = lax.axis_index("ep") * local
    pairs = [(rows_in, rows_ref), (gain_in, gain_ref)]
    for expert in range(local):
        pairs.append((gate_in.at[expert], gate_ref.at[expert]))
        pairs.append((up_in.at[expert], up_ref.at[expert]))
    for expert in range(local):
        part = pl.ds(expert * units, units)
        pairs.append((down_in.at[part], down_ref.at[part]))
    copies = start_all(pairs, sems)
    copies[0].wait()
    copies[1].wait()
    normed[...] = normed_rows(rows_ref, gain_ref)
    for expert in range(local):
        copies[2 + 2 * expert].wait()
        copies[3 + 2 * expert].wait()
        scale = share_of(message_ref, first + expert, tokens)
        fill_hidden(hidden, expert, scale, normed, gate_ref.at[expert], up_ref.at[expert])
    for copy in copies[2 + 2 * local :]:
        copy.wait()
    store_halves(hidden, down_ref, total, seat()[1], (kept_ref, sent_ref))


def own_partial(rows, message, gain, gate_weight, up_weight, down_weight, block):
    tokens, width = rows.shape
    local, _, units = gate_weight.shape
    half = jax.ShapeDtypeStruct((tokens // 2, width), jnp.bfloat16)
    held = [pltpu.VMEM(w.shape, w.dtype) for w in (gate_weight, up_weight, down_weight)]
    return pl.pallas_call(
        own_kernel,
        in_specs=[HBM] * 5 + [VMEM],
        out_specs=[VMEM] * 5,
        out_shape=[half, half] + held,
        scratch_shapes=[
            pltpu.VMEM((1, width), jnp.float32),
            pltpu.VMEM((tokens, width), rows.dtype),
            pltpu.VMEM((tokens, width), jnp.bfloat16),
            pltpu.VMEM((tokens, local * units), jnp.bfloat16),
            pltpu.VMEM((tokens // block, block, width), jnp.bfloat16),
            pltpu.SemaphoreType.DMA((2 + 3 * local,)),
        ],
        compiler_params=pltpu.CompilerParams(vmem_limit_bytes=10 << 20),
        cost_estimate=pl.CostEstimate(
            flops=6 * tokens * width * local * units,
            bytes_accessed=4 * tokens * width + 6 * local * units * width,
            transcendentals=tokens * local * units,
        ),
        name="own",
    )(*from_hbm(gain.reshape(1, width), rows, gate_weight, up_weight, down_weight), message)


def expert_kernel(gate_ref, up_ref, down_ref, *refs, groups):
    inputs, outputs = refs[: 2 * groups], refs[2 * groups : 4 * groups]
    normed, hidden, total = refs[4 * groups :]
    first, core = lax.axis_index("ep") * gate_ref.shape[0], seat()[1]
    half = normed.shape[0] // (2 * groups)
    for group in range(groups):
        mine_ref, other_ref = inputs[2 * group : 2 * group + 2]
        for source, which in ((mine_ref, core), (other_ref, 1 - core)):
            start = pl.multiple_of((2 * group + which) * half, half)
            normed[pl.ds(start, half), :] = source[:half, :]
    for expert in range(gate_ref.shape[0]):
        shares = [share_of(ref, first + expert, 2 * half) for ref in inputs[::2]]
        scale = jnp.concatenate(shares, axis=0)
        fill_hidden(hidden, expert, scale, normed, gate_ref.at[expert], up_ref.at[expert])
    store_halves(hidden, down_ref, total, core, outputs)


def expert_partial(chunks, gate_weight, up_weight, down_weight, block):
    groups = len(chunks)
    half, width = chunks[0][0].shape
    half -= 8
    rows = 2 * half * groups
    local, _, units = gate_weight.shape
    inputs = [array for chunk in chunks for array in chunk]
    outputs = pl.pallas_call(
        lambda *refs: expert_kernel(*refs, groups=groups),
        in_specs=[VMEM] * (3 + len(inputs)),
        out_specs=[VMEM] * (2 * groups),
        out_shape=[jax.ShapeDtypeStruct((half, width), jnp.bfloat16)] * (2 * groups),
        scratch_shapes=[
            pltpu.VMEM((rows, width), jnp.bfloat16),
            pltpu.VMEM((rows, local * units), jnp.bfloat16),
            pltpu.VMEM((rows // block, block, width), jnp.bfloat16),
        ],
        compiler_params=pltpu.CompilerParams(vmem_limit_bytes=16 << 20),
        cost_estimate=pl.CostEstimate(
            flops=6 * rows * width * local * units,
            bytes_accessed=4 * rows * width,
            transcendentals=rows * local * units,
        ),
        name="experts",
    )(gate_weight, up_weight, down_weight, *inputs)
    return [(outputs[2 * g], outputs[2 * g + 1]) for g in range(groups)]


def half_kernel(gate_ref, up_ref, down_ref, *refs, rest):
    inputs, (kept_ref, sent_ref, normed, hidden, total) = refs[:-5], refs[-5:]
    core = seat()[1]
    first = lax.axis_index("ep") * gate_ref.shape[0]
    half = normed.shape[0] // len(inputs)
    side = 1 - core if rest else core
    for group, source in enumerate(inputs):
        normed[group * half : (group + 1) * half, :] = source[:half, :]
    for expert in range(gate_ref.shape[0]):
        shares = [share_of(ref, first + expert, 2 * half) for ref in inputs]
        shares = [jnp.where(side == 0, share[:half], share[half:]) for share in shares]
        scale = jnp.concatenate(shares, axis=0)
        fill_hidden(hidden, expert, scale, normed, gate_ref.at[expert], up_ref.at[expert])
    result = jnp.dot(hidden[...], down_ref[...], preferred_element_type=jnp.float32)
    total[...] = result.astype(jnp.bfloat16).reshape(total.shape)
    blocks, block, _ = total.shape
    for k in range(blocks // CORES):
        rows_of = slice(k * block, (k + 1) * block)
        kept_ref[rows_of, :] = total[CORES * k + core]
        sent_ref[rows_of, :] = total[CORES * k + 1 - core]


def half_partial(inputs, gate_weight, up_weight, down_weight, block, rest):
    half, width = inputs[0].shape
    half -= 8
    rows = len(inputs) * half
    local, _, units = gate_weight.shape
    return pl.pallas_call(
        lambda *refs: half_kernel(*refs, rest=rest),
        in_specs=[VMEM] * (3 + len(inputs)),
        out_specs=[VMEM] * 2,
        out_shape=[jax.ShapeDtypeStruct((rows // CORES, width), jnp.bfloat16)] * 2,
        scratch_shapes=[
            pltpu.VMEM((rows, width), jnp.bfloat16),
            pltpu.VMEM((rows, local * units), jnp.bfloat16),
            pltpu.VMEM((rows // block, block, width), jnp.bfloat16),
        ],
        compiler_params=pltpu.CompilerParams(vmem_limit_bytes=12 << 20),
        cost_estimate=pl.CostEstimate(
            flops=6 * rows * width * local * units,
            bytes_accessed=4 * rows * width,
            transcendentals=rows * local * units,
        ),
        name="halves",
    )(gate_weight, up_weight, down_weight, *inputs)


def join_kernel(kept_mine, kept_rest, back_mine, back_rest, out_ref, *, group):
    half = out_ref.shape[0] // 2
    core = seat()[1]
    here, there = (slice(g * half, (g + 1) * half) for g in (group, 1 - group))
    for kept, back, side in ((kept_mine, back_rest, core), (kept_rest, back_mine, 1 - core)):
        rows_of = pl.ds(pl.multiple_of(side * half, half), half)
        out_ref[rows_of, :] = added(kept[here, :], back[there, :])


def join_halves(kept_mine, kept_rest, back_mine, back_rest, group):
    return pl.pallas_call(
        lambda *refs: join_kernel(*refs, group=group),
        in_specs=[VMEM] * 4,
        out_specs=VMEM,
        out_shape=jax.ShapeDtypeStruct(kept_mine.shape, kept_mine.dtype),
        compiler_params=pltpu.CompilerParams(vmem_limit_bytes=4 << 20),
        name="join",
    )(kept_mine, kept_rest, back_mine, back_rest)


def spread_kernel(early_ref, late_ref, own_ref, *out_refs, start):
    chips, _, width = late_ref.shape
    for step in range(chips):
        at = chip_after(seat()[0], step, chips)
        part = early_ref[at, :, start : start + width] + late_ref[at].astype(jnp.float32)
        if step:
            out_refs[step - 1][...] = part.astype(jnp.bfloat16)
        else:
            own_ref[...] = part


def spread(early, late, start):
    chips, block, width = late.shape
    return pl.pallas_call(
        lambda *refs: spread_kernel(*refs, start=start),
        in_specs=[VMEM, VMEM],
        out_specs=[VMEM] * chips,
        out_shape=[jax.ShapeDtypeStruct((block, width), jnp.float32)]
        + [jax.ShapeDtypeStruct((block, width), jnp.bfloat16)] * (chips - 1),
        cost_estimate=pl.CostEstimate(
            flops=late.size, bytes_accessed=8 * late.size, transcendentals=0
        ),
        compiler_params=pltpu.CompilerParams(vmem_limit_bytes=4 << 20),
        name="spread",
    )(early, late)


def finish_kernel(gain_ref, *refs):
    inputs, out_ref = refs[:-1], refs[-1]
    each = len(inputs) // PIECES
    totals = []
    for piece in range(PIECES):
        own, *parts = inputs[piece * each : (piece + 1) * each]
        total = own[...]
        for part in parts:
            total = total + part[...].astype(jnp.float32)
        totals.append(total)
    total = jnp.concatenate(totals, axis=1)
    out_ref[...] = rms_scale(total, gain_ref[...]).astype(jnp.bfloat16)


def finish(gain, parts):
    block = parts[0].shape[0]
    return pl.pallas_call(
        finish_kernel,
        in_specs=[VMEM] * (1 + len(parts)),
        out_specs=VMEM,
        out_shape=jax.ShapeDtypeStruct((block, gain.shape[0]), jnp.bfloat16),
        compiler_params=pltpu.CompilerParams(vmem_limit_bytes=4 << 20),
        name="finish",
    )(gain.reshape(1, -1), *parts)


def added(left, right):
    return (left.astype(jnp.float32) + right.astype(jnp.float32)).astype(jnp.bfloat16)


def pass_kernel(held_ref, passing_ref, out_ref, *, start):
    held = held_ref[:, start : start + passing_ref.shape[1]]
    out_ref[...] = added(held, passing_ref[...])


def pass_on(held, passing, start):
    return pl.pallas_call(
        lambda *refs: pass_kernel(*refs, start=start),
        in_specs=[VMEM, VMEM],
        out_specs=VMEM,
        out_shape=jax.ShapeDtypeStruct(passing.shape, passing.dtype),
        compiler_params=pltpu.CompilerParams(vmem_limit_bytes=4 << 20),
        name="pass_on",
    )(held, passing)


def dense_experts(
    message, expert_in, pre_gain, gate_weight, up_weight, down_weight, post_gain
):
    tokens, width = expert_in.shape
    chips = lax.axis_size("tp") // CORES
    block = tokens // lax.axis_size("tp")
    from_a = to_group(message, 0)
    from_b = to_group(message, 1)
    weights = (pre_gain, gate_weight, up_weight, down_weight.reshape(-1, width), block)
    kept, sent, *held = own_partial(expert_in, message, *weights)
    weights = (*held, block)
    early = kept.astype(jnp.float32) + to_core(sent).astype(jnp.float32)
    from_c = to_group(from_a, 1)
    other_b = to_core(from_a)
    other_a = to_core(from_b)
    other_c = to_core(from_c)
    kept_mine, sent = half_partial((from_a, from_b), *weights, rest=False)
    back_mine = to_core(sent)
    kept_rest, sent = half_partial((other_a, other_b), *weights, rest=True)
    back_rest = to_core(sent)
    halves = (kept_mine, kept_rest, back_mine, back_rest)
    joined_a = join_halves(*halves, 0)
    joined_b = join_halves(*halves, 1)
    near_sum = to_group(joined_a, 0)
    ((kept_c, sent_c),) = expert_partial([(from_c, other_c)], *weights)
    back_c = to_core(sent_c)
    cut = width * 8 // 16
    columns = [slice(0, cut), slice(cut, width)]
    joined_c = [added(kept_c[:, part], back_c[:, part]) for part in columns]
    passed, late = [], []
    for piece in range(PIECES):
        passing = to_group(joined_c[piece], 0)
        passed.append(pass_on(joined_b, passing, columns[piece].start))
    for piece in range(PIECES):
        late.append(to_group(passed[piece], 1))
    early = lax.optimization_barrier(early + near_sum.astype(jnp.float32))
    early = early.reshape(chips, block, width)
    parts = []
    for piece in range(PIECES):
        own, *pieces = spread(early, late[piece].reshape(chips, block, -1), columns[piece].start)
        parts.append(own)
        for step in range(1, chips):
            parts.append(to_chip(pieces[step - 1], step))
    return finish(post_gain, parts)


def mix_kernel(rim_ref, rows_ref, weight_ref, gain_ref, out_ref):
    rows = rows_ref.shape[0]
    group = rows_ref.shape[1] // len(WINDOWS)
    spare = rim_ref.shape[0]
    device = lax.axis_index("ep") * lax.axis_size("tp") + lax.axis_index("tp")
    position = device * rows + lax.broadcasted_iota(jnp.int32, (rows, 1), 0)
    for which, window in enumerate(WINDOWS):
        cols = slice(which * group, (which + 1) * group)
        rim = jnp.where(device == 0, 0.0, rim_ref[:, cols].astype(jnp.float32))
        values = jnp.concatenate([rim, rows_ref[:, cols].astype(jnp.float32)], axis=0)
        running, reach = values, 1
        while reach < window:
            running = running + pltpu.roll(running, reach, 0)
            reach *= 2
        count = jnp.minimum(position + 1, window).astype(jnp.float32)
        diff = running[spare:] / count - values[spare:]
        mixed = jnp.dot(
            diff.astype(jnp.bfloat16), weight_ref[which], preferred_element_type=jnp.float32
        )
        out_ref[:, cols] = (mixed * gain_ref[:, cols]).astype(jnp.bfloat16)


def mix(rim, rows, weight, gain):
    return pl.pallas_call(
        mix_kernel,
        in_specs=[VMEM] * 4,
        out_specs=VMEM,
        out_shape=jax.ShapeDtypeStruct(rows.shape, jnp.bfloat16),
        compiler_params=pltpu.CompilerParams(vmem_limit_bytes=6 << 20),
        cost_estimate=pl.CostEstimate(
            flops=2 * rows.size * weight.shape[1],
            bytes_accessed=4 * rows.size,
            transcendentals=0,
        ),
        name="mix",
    )(rim, rows, weight, gain.reshape(1, -1))


def join_shards(joined, weights, far):
    chip, core = seat()
    chips = 2 * len(weights) // CORES
    depth = weights[0].shape[0]
    base = lax.div(chip, chips // 2)
    base = (1 - base if far else base) * (chips // 2)
    for k, weight in enumerate(weights):
        step = k // CORES + (chips // 2 if far else 0)
        shard = (chip_before(chip, step, chips) - base) * CORES
        shard = shard + (core if k % CORES == 0 else 1 - core)
        joined[pl.ds(pl.multiple_of(shard * depth, depth), depth), :] = weight[...]
    return base * CORES * depth


def near_kernel(mixed_ref, *refs):
    weights, out_ref, joined = refs[:-2], refs[-2], refs[-1]
    span = joined.shape[0]
    start = pl.multiple_of(join_shards(joined, weights, False), span)
    out_ref[...] = jnp.dot(
        mixed_ref[:, pl.ds(start, span)], joined[...], preferred_element_type=jnp.float32
    )


def near_project(mixed, weights):
    rows, depth = mixed.shape
    width = weights[0].shape[1]
    return pl.pallas_call(
        near_kernel,
        in_specs=[VMEM] * (1 + len(weights)),
        out_specs=VMEM,
        out_shape=pltpu.VMEM((rows, width), jnp.float32),
        scratch_shapes=[pltpu.VMEM((depth // 2, width), jnp.bfloat16)],
        compiler_params=pltpu.CompilerParams(vmem_limit_bytes=8 << 20),
        cost_estimate=pl.CostEstimate(
            flops=rows * depth * width, bytes_accessed=4 * rows * width, transcendentals=0
        ),
        name="near",
    )(mixed, *weights)


def project_kernel(mixed_ref, near_ref, gain_ref, *refs):
    weights, out_ref, joined = refs[:-2], refs[-2], refs[-1]
    span, tile = joined.shape[0], out_ref.shape[0]
    row = pl.multiple_of(pl.program_id(0) * tile, tile)

    @pl.when(pl.program_id(0) == 0)
    def _():
        join_shards(joined, weights, True)

    chip, _ = seat()
    chips = 2 * len(weights) // CORES
    start = pl.multiple_of((1 - lax.div(chip, chips // 2)) * span, span)
    total = near_ref[pl.ds(row, tile), :] + jnp.dot(
        mixed_ref[pl.ds(row, tile), pl.ds(start, span)],
        joined[...],
        preferred_element_type=jnp.float32,
    )
    out_ref[...] = rms_scale(total, gain_ref[...]).astype(jnp.bfloat16)


def project(mixed, near, gain, weights):
    rows, depth = mixed.shape
    width = weights[0].shape[1]
    tile = min(256, rows)
    return pl.pallas_call(
        project_kernel,
        grid=(rows // tile,),
        in_specs=[VMEM] * (3 + len(weights)),
        out_specs=pl.BlockSpec((tile, width), lambda i: (i, 0)),
        out_shape=jax.ShapeDtypeStruct((rows, width), jnp.bfloat16),
        scratch_shapes=[pltpu.VMEM((depth // 2, width), jnp.bfloat16)],
        compiler_params=pltpu.CompilerParams(vmem_limit_bytes=8 << 20),
        cost_estimate=pl.CostEstimate(
            flops=rows * depth * width,
            bytes_accessed=6 * rows * width,
            transcendentals=0,
        ),
        name="project",
    )(mixed, near, gain.reshape(1, width), *weights)


def step(
    pool_in,
    pool_weight,
    pool_gain,
    out_weight,
    mix_gain,
    expert_in,
    routes,
    route_weight,
    pre_gain,
    gate_weight,
    up_weight,
    down_weight,
    post_gain,
):
    rows, _ = pool_in.shape
    ep_count, tp_count = lax.axis_size("ep"), lax.axis_size("tp")
    chips = tp_count // CORES
    tokens_here, choose = routes.shape
    block_tokens = tokens_here // tp_count
    capacity = 2 * block_tokens * choose // (gate_weight.shape[0] * ep_count)
    experts_in_all = gate_weight.shape[0] * ep_count
    dense = capacity >= block_tokens and ep_count == 4
    dense = dense and experts_in_all * tokens_here <= expert_in.shape[1]
    tail = pool_in[rows - REACH :]
    if dense:
        message, tail = pack(
            expert_in, pre_gain, routes, route_weight, pool_in
        )
    rim = to_next(tail)
    if dense:
        expert_out = dense_experts(
            message, expert_in, pre_gain, gate_weight, up_weight, down_weight, post_gain
        )
    else:
        expert_out = routed_experts(
            expert_in, routes, route_weight, pre_gain, gate_weight, up_weight, down_weight,
            post_gain,
        )
    shards, held = [], [out_weight]
    for step in range(1, chips):
        longer = step & (step - 1) if paired(chips) else 0
        held.append(to_chip(held[longer], step ^ longer))
    for shard in held:
        shards += [shard, to_core(shard)]
    mixed = mix(rim, pool_in, pool_weight, pool_gain)
    half = len(shards) // 2
    mix_out = project(mixed, near_project(mixed, shards[:half]), mix_gain, shards[half:])
    return (mix_out, expert_out)


def solution(mesh):
    return jax.shard_map(
        step,
        mesh=mesh,
        in_specs=(
            P(("ep", "tp"), None),
            P(),
            P(),
            P("tp", None),
            P(),
            P("ep", None),
            P("ep", None),
            P("ep", None),
            P(),
            P("ep", None, "tp"),
            P("ep", None, "tp"),
            P("ep", "tp", None),
            P(),
        ),
        out_specs=(P(("ep", "tp"), None), P(("ep", "tp"), None)),
        check_vma=False,
    )
```

```python
import jax
import jax.numpy as jnp
from jax import lax
from jax.experimental import pallas as pl
from jax.experimental.pallas import tpu as pltpu
from jax.sharding import PartitionSpec as P


WINDOWS = (2, 4, 8, 16)
EPS = 1e-06
LIMIT = 7.0
ALPHA = 1.702
CORES = 2
PIECES = 2
REACH = max(WINDOWS)


def to_next(block):
    eps, tps = lax.axis_size("ep"), lax.axis_size("tp")
    return moved(block, lambda e, t: ((e + (t + 1) // tps) % eps, (t + 1) % tps))


def moved(block, target):
    eps, tps = lax.axis_size("ep"), lax.axis_size("tp")
    route = []
    for e in range(eps):
        for t in range(tps):
            te, tt = target(e, t)
            route.append((e * tps + t, te * tps + tt))
    return lax.ppermute(block, ("ep", "tp"), route)


def to_core(block):
    return moved(block, lambda e, t: (e, t ^ 1))


def to_group(block, turn):
    masks = (1, 2) if turn == 0 else (2, 1)
    return moved(block, lambda e, t: (e ^ masks[t % CORES], t))


def paired(chips):
    return chips & (chips - 1) == 0


def to_chip(block, step):
    chips = lax.axis_size("tp") // CORES
    target = (lambda z: z ^ step) if paired(chips) else (lambda z: (z + step) % chips)
    return moved(block, lambda e, t: (e, target(t // CORES) * CORES + t % CORES))


def chip_after(chip, step, chips):
    return lax.bitwise_xor(chip, step) if paired(chips) else lax.rem(chip + step, chips)


def chip_before(chip, step, chips):
    return lax.bitwise_xor(chip, step) if paired(chips) else lax.rem(chip + chips - step, chips)


def rms_scale(values, gain):
    mean_square = jnp.mean(values * values, axis=-1, keepdims=True)
    return values * lax.rsqrt(mean_square + EPS) * gain


def selection(block_routes, experts, capacity):
    flat = block_routes.reshape(-1)
    onehot = (flat[:, None] == jnp.arange(experts, dtype=jnp.int32)[None, :]).astype(jnp.int32)
    earlier = jnp.cumsum(onehot, axis=0) - onehot
    rank = jnp.sum(earlier * onehot, axis=1)
    slots = (flat * capacity + rank).reshape(block_routes.shape)
    return (
        slots[:, :, None] == jnp.arange(experts * capacity, dtype=jnp.int32)[None, None, :]
    ).astype(jnp.bfloat16)


def clamped_unit(gate, up):
    gate = jnp.minimum(gate, LIMIT)
    up = jnp.clip(up, -LIMIT, LIMIT)
    return (up + 1.0) * gate * jax.nn.sigmoid(ALPHA * gate)


def hidden_rows(arrived, gate_weight, up_weight):
    gate = jnp.einsum("necd,edf->necf", arrived, gate_weight, preferred_element_type=jnp.float32)
    up = jnp.einsum("necd,edf->necf", arrived, up_weight, preferred_element_type=jnp.float32)
    return clamped_unit(gate, up).astype(jnp.bfloat16)


def routed_experts(
    expert_in, routes, route_weight, pre_gain, gate_weight, up_weight, down_weight, post_gain
):
    width = expert_in.shape[1]
    ep_count = lax.axis_size("ep")
    tp_count = lax.axis_size("tp")
    tp_place = lax.axis_index("tp")
    local_experts = gate_weight.shape[0]
    experts = local_experts * ep_count
    tokens_here, choose = routes.shape
    block_tokens = tokens_here // tp_count
    capacity = 2 * block_tokens * choose // experts
    block_routes = lax.dynamic_slice_in_dim(routes, tp_place * block_tokens, block_tokens, 0)
    block_rows = lax.dynamic_slice_in_dim(expert_in, tp_place * block_tokens, block_tokens, 0)
    normed = rms_scale(block_rows.astype(jnp.float32), pre_gain).astype(jnp.bfloat16)
    own_picks = selection(block_routes, experts, capacity)
    buffer = jnp.einsum(
        "ts,td->sd", jnp.sum(own_picks, axis=1), normed, preferred_element_type=jnp.float32
    ).astype(jnp.bfloat16)
    buffer = buffer.reshape(ep_count, local_experts, capacity, width)
    arrived = lax.all_to_all(buffer, "ep", split_axis=0, concat_axis=0, tiled=True)
    hidden_all = hidden_rows(
        lax.all_gather(arrived, "tp", axis=0, tiled=True), gate_weight, up_weight
    )
    summed = lax.psum_scatter(
        jnp.einsum(
            "necf,efd->necd", hidden_all, down_weight, preferred_element_type=jnp.float32
        ).astype(jnp.bfloat16),
        "tp",
        scatter_dimension=0,
        tiled=True,
    )
    returned = lax.all_to_all(summed, "ep", split_axis=0, concat_axis=0, tiled=True)
    returned = returned.reshape(experts * capacity, width)
    per_route = jnp.einsum("tks,sd->tkd", own_picks, returned, preferred_element_type=jnp.float32)
    weights = lax.dynamic_slice_in_dim(route_weight, tp_place * block_tokens, block_tokens, 0)
    combined = jnp.sum(per_route * weights[:, :, None], axis=1)
    return rms_scale(combined, post_gain).astype(jnp.bfloat16)


def seat():
    place = lax.axis_index("tp")
    return lax.div(place, CORES), lax.rem(place, CORES)


VMEM = pl.BlockSpec(memory_space=pltpu.VMEM)
HBM = pl.BlockSpec(memory_space=pltpu.HBM)


def normed_rows(source, gain):
    return rms_scale(source[...].astype(jnp.float32), gain[...]).astype(jnp.bfloat16)


def share_of(message, expert, tokens):
    start = pl.multiple_of(expert * tokens, tokens)
    notes = message[tokens // CORES :, pl.ds(start, tokens)].astype(jnp.float32)
    notes = jnp.transpose(notes)
    return notes[:, 0:1] + notes[:, 1:2]


def fill_hidden(hidden, expert, scale, normed, gate_weight, up_weight):
    units = gate_weight.shape[1]
    gate = jnp.dot(normed[...], gate_weight[...], preferred_element_type=jnp.float32)
    up = jnp.dot(normed[...], up_weight[...], preferred_element_type=jnp.float32)
    hidden[:, expert * units : (expert + 1) * units] = (clamped_unit(gate, up) * scale).astype(
        jnp.bfloat16
    )


def store_halves(hidden, down_weight, total, core, outputs, cols=slice(None)):
    result = jnp.dot(hidden[...], down_weight[:, cols], preferred_element_type=jnp.float32)
    total[...] = result.astype(jnp.bfloat16).reshape(total.shape)
    groups = len(outputs) // 2
    chips = total.shape[0] // (CORES * groups)
    block = total.shape[1]
    for group in range(groups):
        for chip in range(chips):
            start = CORES * (group * chips + chip)
            rows_of = slice(chip * block, (chip + 1) * block)
            outputs[2 * group][rows_of, :] = total[start + core]
            outputs[2 * group + 1][rows_of, :] = total[start + 1 - core]


def start_all(pairs, sems):
    copies = [
        pltpu.make_async_copy(source, target, sems.at[k])
        for k, (source, target) in enumerate(pairs)
    ]
    for copy in copies:
        copy.start()
    return copies


def from_hbm(*arrays):
    return [pltpu.with_memory_space_constraint(array, pltpu.HBM) for array in arrays]


def pack_kernel(
    rows_in, gain_in, routes_in, weight_in, pool_in,
    message_ref, tail_ref, rows_ref, gain_ref, routes_ref, weight_ref, sems,
):
    half = rows_ref.shape[0]
    tokens = routes_ref.shape[1]
    experts = message_ref.shape[1] // tokens
    start = pl.multiple_of(seat()[1] * half, half)
    copies = start_all(
        [
            (routes_in, routes_ref),
            (weight_in, weight_ref),
            (gain_in, gain_ref),
            (rows_in.at[pl.ds(start, half)], rows_ref),
            (pool_in.at[pl.ds(pool_in.shape[0] - REACH, REACH)], tail_ref),
        ],
        sems,
    )
    copies[0].wait()
    copies[1].wait()
    notes = message_ref.shape[0] - half
    line = lax.broadcasted_iota(jnp.int32, (notes, tokens), 0)
    for expert in range(experts):
        share = jnp.sum(
            jnp.where(routes_ref[...] == expert, weight_ref[...], 0.0), axis=0, keepdims=True
        )
        coarse = share.astype(jnp.bfloat16).astype(jnp.float32)
        both = jnp.where(line == 0, coarse, jnp.where(line == 1, share - coarse, 0.0))
        message_ref[half:, expert * tokens : (expert + 1) * tokens] = both.astype(jnp.bfloat16)
    copies[2].wait()
    copies[3].wait()
    message_ref[:half, :] = normed_rows(rows_ref, gain_ref)
    copies[4].wait()


def pack(rows, gain, routes, route_weight, pool_in):
    tokens, width = rows.shape
    choose = routes.shape[1]
    return pl.pallas_call(
        pack_kernel,
        in_specs=[HBM] * 5,
        out_specs=[VMEM] * 2,
        out_shape=[
            jax.ShapeDtypeStruct((tokens // CORES + 8, width), rows.dtype),
            jax.ShapeDtypeStruct((REACH, pool_in.shape[1]), pool_in.dtype),
        ],
        scratch_shapes=[
            pltpu.VMEM((tokens // CORES, width), rows.dtype),
            pltpu.VMEM((1, width), jnp.float32),
            pltpu.VMEM((choose, tokens), jnp.int32),
            pltpu.VMEM((choose, tokens), jnp.float32),
            pltpu.SemaphoreType.DMA((5,)),
        ],
        compiler_params=pltpu.CompilerParams(vmem_limit_bytes=3 << 20),
        name="pack",
    )(*from_hbm(rows, gain.reshape(1, width), routes.T, route_weight.T, pool_in))


def own_kernel(
    gain_in, rows_in, gate_in, up_in, down_in, message_ref,
    kept_ref, sent_ref, gate_ref, up_ref, down_ref,
    gain_ref, rows_ref, normed, hidden, total, sems,
):
    local, _, units = gate_ref.shape
    tokens = rows_ref.shape[0]
    first = lax.axis_index("ep") * local
    pairs = [(rows_in, rows_ref), (gain_in, gain_ref)]
    for expert in range(local):
        pairs.append((gate_in.at[expert], gate_ref.at[expert]))
        pairs.append((up_in.at[expert], up_ref.at[expert]))
    for expert in range(local):
        part = pl.ds(expert * units, units)
        pairs.append((down_in.at[part], down_ref.at[part]))
    copies = start_all(pairs, sems)
    copies[0].wait()
    copies[1].wait()
    normed[...] = normed_rows(rows_ref, gain_ref)
    for expert in range(local):
        copies[2 + 2 * expert].wait()
        copies[3 + 2 * expert].wait()
        scale = share_of(message_ref, first + expert, tokens)
        fill_hidden(hidden, expert, scale, normed, gate_ref.at[expert], up_ref.at[expert])
    for copy in copies[2 + 2 * local :]:
        copy.wait()
    store_halves(hidden, down_ref, total, seat()[1], (kept_ref, sent_ref))


def own_partial(rows, message, gain, gate_weight, up_weight, down_weight, block):
    tokens, width = rows.shape
    local, _, units = gate_weight.shape
    half = jax.ShapeDtypeStruct((tokens // 2, width), jnp.bfloat16)
    held = [pltpu.VMEM(w.shape, w.dtype) for w in (gate_weight, up_weight, down_weight)]
    return pl.pallas_call(
        own_kernel,
        in_specs=[HBM] * 5 + [VMEM],
        out_specs=[VMEM] * 5,
        out_shape=[half, half] + held,
        scratch_shapes=[
            pltpu.VMEM((1, width), jnp.float32),
            pltpu.VMEM((tokens, width), rows.dtype),
            pltpu.VMEM((tokens, width), jnp.bfloat16),
            pltpu.VMEM((tokens, local * units), jnp.bfloat16),
            pltpu.VMEM((tokens // block, block, width), jnp.bfloat16),
            pltpu.SemaphoreType.DMA((2 + 3 * local,)),
        ],
        compiler_params=pltpu.CompilerParams(vmem_limit_bytes=10 << 20),
        cost_estimate=pl.CostEstimate(
            flops=6 * tokens * width * local * units,
            bytes_accessed=4 * tokens * width + 6 * local * units * width,
            transcendentals=tokens * local * units,
        ),
        name="own",
    )(*from_hbm(gain.reshape(1, width), rows, gate_weight, up_weight, down_weight), message)


def far_kernel(
    gate_ref, up_ref, down_ref, mine_ref, other_ref, hidden_ref, kept_ref, sent_ref, normed, total,
    *, cols,
):
    first, core = lax.axis_index("ep") * gate_ref.shape[0], seat()[1]
    half = normed.shape[0] // 2
    for source, which in ((mine_ref, core), (other_ref, 1 - core)):
        start = pl.multiple_of(which * half, half)
        normed[pl.ds(start, half), :] = source[:half, :]
    for expert in range(gate_ref.shape[0]):
        scale = share_of(mine_ref, first + expert, 2 * half)
        fill_hidden(hidden_ref, expert, scale, normed, gate_ref.at[expert], up_ref.at[expert])
    store_halves(hidden_ref, down_ref, total, core, (kept_ref, sent_ref), cols)


def far_partial(mine, other, gate_weight, up_weight, down_weight, block, cols):
    half, width = mine.shape
    half -= 8
    rows, span = 2 * half, cols.stop - cols.start
    local, _, units = gate_weight.shape
    part = jax.ShapeDtypeStruct((half, span), jnp.bfloat16)
    return pl.pallas_call(
        lambda *refs: far_kernel(*refs, cols=cols),
        in_specs=[VMEM] * 5,
        out_specs=[VMEM] * 3,
        out_shape=[pltpu.VMEM((rows, local * units), jnp.bfloat16), part, part],
        scratch_shapes=[
            pltpu.VMEM((rows, width), jnp.bfloat16),
            pltpu.VMEM((rows // block, block, span), jnp.bfloat16),
        ],
        compiler_params=pltpu.CompilerParams(vmem_limit_bytes=12 << 20),
        cost_estimate=pl.CostEstimate(
            flops=5 * rows * width * local * units,
            bytes_accessed=4 * rows * width,
            transcendentals=rows * local * units,
        ),
        name="far",
    )(gate_weight, up_weight, down_weight, mine, other)


def down_kernel(hidden_ref, down_ref, kept_ref, sent_ref, total, *, cols):
    store_halves(hidden_ref, down_ref, total, seat()[1], (kept_ref, sent_ref), cols)


def down_partial(hidden, down_weight, block, cols):
    rows, span = hidden.shape[0], cols.stop - cols.start
    part = jax.ShapeDtypeStruct((rows // 2, span), jnp.bfloat16)
    return pl.pallas_call(
        lambda *refs: down_kernel(*refs, cols=cols),
        in_specs=[VMEM] * 2,
        out_specs=[VMEM] * 2,
        out_shape=[part, part],
        scratch_shapes=[pltpu.VMEM((rows // block, block, span), jnp.bfloat16)],
        compiler_params=pltpu.CompilerParams(vmem_limit_bytes=8 << 20),
        cost_estimate=pl.CostEstimate(
            flops=2 * rows * span * hidden.shape[1],
            bytes_accessed=4 * rows * span,
            transcendentals=0,
        ),
        name="down",
    )(hidden, down_weight)


def half_kernel(gate_ref, up_ref, down_ref, *refs, rest):
    inputs, (kept_ref, sent_ref, normed, hidden, total) = refs[:-5], refs[-5:]
    core = seat()[1]
    first = lax.axis_index("ep") * gate_ref.shape[0]
    half = normed.shape[0] // len(inputs)
    side = 1 - core if rest else core
    for group, source in enumerate(inputs):
        normed[group * half : (group + 1) * half, :] = source[:half, :]
    for expert in range(gate_ref.shape[0]):
        shares = [share_of(ref, first + expert, 2 * half) for ref in inputs]
        shares = [jnp.where(side == 0, share[:half], share[half:]) for share in shares]
        scale = jnp.concatenate(shares, axis=0)
        fill_hidden(hidden, expert, scale, normed, gate_ref.at[expert], up_ref.at[expert])
    result = jnp.dot(hidden[...], down_ref[...], preferred_element_type=jnp.float32)
    total[...] = result.astype(jnp.bfloat16).reshape(total.shape)
    blocks, block, _ = total.shape
    for k in range(blocks // CORES):
        rows_of = slice(k * block, (k + 1) * block)
        kept_ref[rows_of, :] = total[CORES * k + core]
        sent_ref[rows_of, :] = total[CORES * k + 1 - core]


def half_partial(inputs, gate_weight, up_weight, down_weight, block, rest):
    half, width = inputs[0].shape
    half -= 8
    rows = len(inputs) * half
    local, _, units = gate_weight.shape
    return pl.pallas_call(
        lambda *refs: half_kernel(*refs, rest=rest),
        in_specs=[VMEM] * (3 + len(inputs)),
        out_specs=[VMEM] * 2,
        out_shape=[jax.ShapeDtypeStruct((rows // CORES, width), jnp.bfloat16)] * 2,
        scratch_shapes=[
            pltpu.VMEM((rows, width), jnp.bfloat16),
            pltpu.VMEM((rows, local * units), jnp.bfloat16),
            pltpu.VMEM((rows // block, block, width), jnp.bfloat16),
        ],
        compiler_params=pltpu.CompilerParams(vmem_limit_bytes=12 << 20),
        cost_estimate=pl.CostEstimate(
            flops=6 * rows * width * local * units,
            bytes_accessed=4 * rows * width,
            transcendentals=rows * local * units,
        ),
        name="halves",
    )(gate_weight, up_weight, down_weight, *inputs)


def join_kernel(kept_mine, kept_rest, back_mine, back_rest, out_ref, *, group):
    half = out_ref.shape[0] // 2
    core = seat()[1]
    here, there = (slice(g * half, (g + 1) * half) for g in (group, 1 - group))
    for kept, back, side in ((kept_mine, back_rest, core), (kept_rest, back_mine, 1 - core)):
        rows_of = pl.ds(pl.multiple_of(side * half, half), half)
        out_ref[rows_of, :] = added(kept[here, :], back[there, :])


def join_halves(kept_mine, kept_rest, back_mine, back_rest, group):
    return pl.pallas_call(
        lambda *refs: join_kernel(*refs, group=group),
        in_specs=[VMEM] * 4,
        out_specs=VMEM,
        out_shape=jax.ShapeDtypeStruct(kept_mine.shape, kept_mine.dtype),
        compiler_params=pltpu.CompilerParams(vmem_limit_bytes=4 << 20),
        name="join",
    )(kept_mine, kept_rest, back_mine, back_rest)


def spread_kernel(early_ref, late_ref, own_ref, *out_refs, start):
    chips, _, width = late_ref.shape
    for step in range(chips):
        at = chip_after(seat()[0], step, chips)
        part = early_ref[at, :, start : start + width] + late_ref[at].astype(jnp.float32)
        if step:
            out_refs[step - 1][...] = part.astype(jnp.bfloat16)
        else:
            own_ref[...] = part


def spread(early, late, start):
    chips, block, width = late.shape
    return pl.pallas_call(
        lambda *refs: spread_kernel(*refs, start=start),
        in_specs=[VMEM, VMEM],
        out_specs=[VMEM] * chips,
        out_shape=[jax.ShapeDtypeStruct((block, width), jnp.float32)]
        + [jax.ShapeDtypeStruct((block, width), jnp.bfloat16)] * (chips - 1),
        cost_estimate=pl.CostEstimate(
            flops=late.size, bytes_accessed=8 * late.size, transcendentals=0
        ),
        compiler_params=pltpu.CompilerParams(vmem_limit_bytes=4 << 20),
        name="spread",
    )(early, late)


def finish_kernel(gain_ref, *refs):
    inputs, out_ref = refs[:-1], refs[-1]
    each = len(inputs) // PIECES
    totals = []
    for piece in range(PIECES):
        own, *parts = inputs[piece * each : (piece + 1) * each]
        total = own[...]
        for part in parts:
            total = total + part[...].astype(jnp.float32)
        totals.append(total)
    total = jnp.concatenate(totals, axis=1)
    out_ref[...] = rms_scale(total, gain_ref[...]).astype(jnp.bfloat16)


def finish(gain, parts):
    block = parts[0].shape[0]
    return pl.pallas_call(
        finish_kernel,
        in_specs=[VMEM] * (1 + len(parts)),
        out_specs=VMEM,
        out_shape=jax.ShapeDtypeStruct((block, gain.shape[0]), jnp.bfloat16),
        compiler_params=pltpu.CompilerParams(vmem_limit_bytes=4 << 20),
        name="finish",
    )(gain.reshape(1, -1), *parts)


def added(left, right):
    return (left.astype(jnp.float32) + right.astype(jnp.float32)).astype(jnp.bfloat16)


def pass_kernel(held_ref, passing_ref, out_ref, *, start):
    held = held_ref[:, start : start + passing_ref.shape[1]]
    out_ref[...] = added(held, passing_ref[...])


def pass_on(held, passing, start):
    return pl.pallas_call(
        lambda *refs: pass_kernel(*refs, start=start),
        in_specs=[VMEM, VMEM],
        out_specs=VMEM,
        out_shape=jax.ShapeDtypeStruct(passing.shape, passing.dtype),
        compiler_params=pltpu.CompilerParams(vmem_limit_bytes=4 << 20),
        name="pass_on",
    )(held, passing)


def dense_experts(
    message, expert_in, pre_gain, gate_weight, up_weight, down_weight, post_gain
):
    tokens, width = expert_in.shape
    chips = lax.axis_size("tp") // CORES
    block = tokens // lax.axis_size("tp")
    from_a = to_group(message, 0)
    from_b = to_group(message, 1)
    weights = (pre_gain, gate_weight, up_weight, down_weight.reshape(-1, width), block)
    kept, sent, *held = own_partial(expert_in, message, *weights)
    weights = (*held, block)
    early = kept.astype(jnp.float32) + to_core(sent).astype(jnp.float32)
    from_c = to_group(from_a, 1)
    other_b = to_core(from_a)
    other_a = to_core(from_b)
    other_c = to_core(from_c)
    kept_mine, sent = half_partial((from_a, from_b), *weights, rest=False)
    back_mine = to_core(sent)
    kept_rest, sent = half_partial((other_a, other_b), *weights, rest=True)
    back_rest = to_core(sent)
    halves = (kept_mine, kept_rest, back_mine, back_rest)
    joined_a = join_halves(*halves, 0)
    joined_b = join_halves(*halves, 1)
    near_sum = to_group(joined_a, 0)
    cut = width // 2
    columns = [slice(0, cut), slice(cut, width)]
    hidden, *first_half = far_partial(from_c, other_c, *weights, columns[0])
    second_half = down_partial(hidden, weights[2], block, columns[1])
    joined_c = []
    for kept_c, sent_c in (first_half, second_half):
        back_c = to_core(sent_c)
        joined_c.append(pass_on(kept_c, back_c, 0))
    passed, late = [], []
    for piece in range(PIECES):
        passing = to_group(joined_c[piece], 0)
        passed.append(pass_on(joined_b, passing, columns[piece].start))
    for piece in range(PIECES):
        late.append(to_group(passed[piece], 1))
    early = lax.optimization_barrier(early + near_sum.astype(jnp.float32))
    early = early.reshape(chips, block, width)
    parts = []
    for piece in range(PIECES):
        own, *pieces = spread(early, late[piece].reshape(chips, block, -1), columns[piece].start)
        parts.append(own)
        for step in range(1, chips):
            parts.append(to_chip(pieces[step - 1], step))
    return finish(post_gain, parts)


def mix_kernel(rim_ref, rows_ref, weight_ref, gain_ref, out_ref):
    rows = rows_ref.shape[0]
    group = rows_ref.shape[1] // len(WINDOWS)
    spare = rim_ref.shape[0]
    device = lax.axis_index("ep") * lax.axis_size("tp") + lax.axis_index("tp")
    position = device * rows + lax.broadcasted_iota(jnp.int32, (rows, 1), 0)
    for which, window in enumerate(WINDOWS):
        cols = slice(which * group, (which + 1) * group)
        rim = jnp.where(device == 0, 0.0, rim_ref[:, cols].astype(jnp.float32))
        values = jnp.concatenate([rim, rows_ref[:, cols].astype(jnp.float32)], axis=0)
        running, reach = values, 1
        while reach < window:
            running = running + pltpu.roll(running, reach, 0)
            reach *= 2
        count = jnp.minimum(position + 1, window).astype(jnp.float32)
        diff = running[spare:] / count - values[spare:]
        mixed = jnp.dot(
            diff.astype(jnp.bfloat16), weight_ref[which], preferred_element_type=jnp.float32
        )
        out_ref[:, cols] = (mixed * gain_ref[:, cols]).astype(jnp.bfloat16)


def mix(rim, rows, weight, gain):
    return pl.pallas_call(
        mix_kernel,
        in_specs=[VMEM] * 4,
        out_specs=VMEM,
        out_shape=jax.ShapeDtypeStruct(rows.shape, jnp.bfloat16),
        compiler_params=pltpu.CompilerParams(vmem_limit_bytes=6 << 20),
        cost_estimate=pl.CostEstimate(
            flops=2 * rows.size * weight.shape[1],
            bytes_accessed=4 * rows.size,
            transcendentals=0,
        ),
        name="mix",
    )(rim, rows, weight, gain.reshape(1, -1))


def join_shards(joined, weights, far):
    chip, core = seat()
    chips = 2 * len(weights) // CORES
    depth = weights[0].shape[0]
    base = lax.div(chip, chips // 2)
    base = (1 - base if far else base) * (chips // 2)
    for k, weight in enumerate(weights):
        step = k // CORES + (chips // 2 if far else 0)
        shard = (chip_before(chip, step, chips) - base) * CORES
        shard = shard + (core if k % CORES == 0 else 1 - core)
        joined[pl.ds(pl.multiple_of(shard * depth, depth), depth), :] = weight[...]
    return base * CORES * depth


def near_kernel(mixed_ref, *refs):
    weights, out_ref, joined = refs[:-2], refs[-2], refs[-1]
    span = joined.shape[0]
    start = pl.multiple_of(join_shards(joined, weights, False), span)
    out_ref[...] = jnp.dot(
        mixed_ref[:, pl.ds(start, span)], joined[...], preferred_element_type=jnp.float32
    )


def near_project(mixed, weights):
    rows, depth = mixed.shape
    width = weights[0].shape[1]
    return pl.pallas_call(
        near_kernel,
        in_specs=[VMEM] * (1 + len(weights)),
        out_specs=VMEM,
        out_shape=pltpu.VMEM((rows, width), jnp.float32),
        scratch_shapes=[pltpu.VMEM((depth // 2, width), jnp.bfloat16)],
        compiler_params=pltpu.CompilerParams(vmem_limit_bytes=8 << 20),
        cost_estimate=pl.CostEstimate(
            flops=rows * depth * width, bytes_accessed=4 * rows * width, transcendentals=0
        ),
        name="near",
    )(mixed, *weights)


def project_kernel(mixed_ref, near_ref, gain_ref, *refs):
    weights, out_ref, joined = refs[:-2], refs[-2], refs[-1]
    span, tile = joined.shape[0], out_ref.shape[0]
    row = pl.multiple_of(pl.program_id(0) * tile, tile)

    @pl.when(pl.program_id(0) == 0)
    def _():
        join_shards(joined, weights, True)

    chip, _ = seat()
    chips = 2 * len(weights) // CORES
    start = pl.multiple_of((1 - lax.div(chip, chips // 2)) * span, span)
    total = near_ref[pl.ds(row, tile), :] + jnp.dot(
        mixed_ref[pl.ds(row, tile), pl.ds(start, span)],
        joined[...],
        preferred_element_type=jnp.float32,
    )
    out_ref[...] = rms_scale(total, gain_ref[...]).astype(jnp.bfloat16)


def project(mixed, near, gain, weights):
    rows, depth = mixed.shape
    width = weights[0].shape[1]
    tile = min(256, rows)
    return pl.pallas_call(
        project_kernel,
        grid=(rows // tile,),
        in_specs=[VMEM] * (3 + len(weights)),
        out_specs=pl.BlockSpec((tile, width), lambda i: (i, 0)),
        out_shape=jax.ShapeDtypeStruct((rows, width), jnp.bfloat16),
        scratch_shapes=[pltpu.VMEM((depth // 2, width), jnp.bfloat16)],
        compiler_params=pltpu.CompilerParams(vmem_limit_bytes=8 << 20),
        cost_estimate=pl.CostEstimate(
            flops=rows * depth * width,
            bytes_accessed=6 * rows * width,
            transcendentals=0,
        ),
        name="project",
    )(mixed, near, gain.reshape(1, width), *weights)


def step(
    pool_in,
    pool_weight,
    pool_gain,
    out_weight,
    mix_gain,
    expert_in,
    routes,
    route_weight,
    pre_gain,
    gate_weight,
    up_weight,
    down_weight,
    post_gain,
):
    rows, _ = pool_in.shape
    ep_count, tp_count = lax.axis_size("ep"), lax.axis_size("tp")
    chips = tp_count // CORES
    tokens_here, choose = routes.shape
    block_tokens = tokens_here // tp_count
    capacity = 2 * block_tokens * choose // (gate_weight.shape[0] * ep_count)
    experts_in_all = gate_weight.shape[0] * ep_count
    dense = capacity >= block_tokens and ep_count == 4
    dense = dense and experts_in_all * tokens_here <= expert_in.shape[1]
    tail = pool_in[rows - REACH :]
    if dense:
        message, tail = pack(
            expert_in, pre_gain, routes, route_weight, pool_in
        )
    rim = to_next(tail)
    if dense:
        expert_out = dense_experts(
            message, expert_in, pre_gain, gate_weight, up_weight, down_weight, post_gain
        )
    else:
        expert_out = routed_experts(
            expert_in, routes, route_weight, pre_gain, gate_weight, up_weight, down_weight,
            post_gain,
        )
    shards, held = [], [out_weight]
    for step in range(1, chips):
        longer = step & (step - 1) if paired(chips) else 0
        held.append(to_chip(held[longer], step ^ longer))
    for shard in held:
        shards += [shard, to_core(shard)]
    mixed = mix(rim, pool_in, pool_weight, pool_gain)
    half = len(shards) // 2
    mix_out = project(mixed, near_project(mixed, shards[:half]), mix_gain, shards[half:])
    return (mix_out, expert_out)


def solution(mesh):
    return jax.shard_map(
        step,
        mesh=mesh,
        in_specs=(
            P(("ep", "tp"), None),
            P(),
            P(),
            P("tp", None),
            P(),
            P("ep", None),
            P("ep", None),
            P("ep", None),
            P(),
            P("ep", None, "tp"),
            P("ep", None, "tp"),
            P("ep", "tp", None),
            P(),
        ),
        out_specs=(P(("ep", "tp"), None), P(("ep", "tp"), None)),
        check_vma=False,
    )
```
